256 devices in a mesh: st: 64 (over z, y, core), tp: 4 (over x).
Axes of the slice: x: 4, y: 4, z: 8, core: 2. Of those that a mesh axis runs over, the one named last changes fastest.
Arguments:
- queries: bfloat16 [65536, 1024], P('st', 'tp'), may hold values from -540 to 540
- gate_pre: bfloat16 [65536, 1024], P('st', 'tp'), may hold values from -6 to 6
- cotangent: bfloat16 [65536, 1024], P('st', 'tp'), may hold values from -6 to 6
- store: bfloat16 [81920, 2048], P('st'), may hold values from -6 to 6
- store_gain: float32 [2048], replicated, may hold values from 0.1 to 1.9
- w_key: bfloat16 [2048, 1024], P(None, 'tp'), may hold values from -0.125 to 0.125
- w_value: bfloat16 [2048, 1024], P(None, 'tp'), may hold values from -0.125 to 0.125
- owners: int32 [512, 4], P('st'), may hold values from 0 to 63, all different within a row; in each aligned block of 8 rows (0 to 7, 8 to 15, ...) at most 1 rows name the same one
- slots: int32 [512, 4], P('st'), may hold values from 0 to 19
Outputs:
- grad_queries: float32 [65536, 1024], P('st', 'tp')
- grad_store: float32 [81920, 2048], P(('st', 'tp'))
- grad_w_value: float32 [2048, 1024], P('st', 'tp')
The draws below stay inside these ranges and needn't reach their ends.
Inputs may be any that keep to these rules, and one draw needn't show every extreme that they name: Each block names 4 different owners. Among the blocks of one device no owner is named twice.
All inputs are finite; a program needn't handle non-finite values.
Results may differ from the reference program's by a relative error of at most 0.014.
Values may be sent and summed in bfloat16 or wider, within the bound.
A program may use at most 192 MiB of HBM per device.

```python
import math
import jax
import jax.numpy as jnp
import numpy as np
from jax import lax

D = 2048
HEADS = 8
HD = 128
PLEN = 64
BLK = 128
NPB = 4
PASS_DEV = 20
XW = 1024
BLK_DEV = 8
CAP = 1
TOKENS = 65536
BLOCKS = 512
PASSAGES = 1280
ROWS = 81920
N_ST = 64


def draw_queries(key, part):
    first_key = jax.random.fold_in(key, 11)
    drawn = jnp.clip(jax.random.normal(first_key, (TOKENS, XW), jnp.float32), -6.0, 6.0)
    return drawn.astype(jnp.bfloat16)


def draw_cotangent(key, part):
    first_key = jax.random.fold_in(key, 13)
    drawn = jnp.clip(jax.random.normal(first_key, (TOKENS, XW), jnp.float32), -6.0, 6.0)
    return drawn.astype(jnp.bfloat16)


def set_ends(array, stream_key, least, high):
    place = [jax.random.randint(jax.random.fold_in(stream_key, axis), (), 0, length) for axis, length in enumerate(array.shape)]
    widest = array.shape.index(max(array.shape))
    neighbour = place[:widest] + [(place[widest] + 1) % array.shape[widest]] + place[widest + 1:]
    return array.at[tuple(place)].set(least).at[tuple(neighbour)].set(high)


def shard_levels(key, extent, shards, low, largest):
    gain = 1.0
    for position, shards_of in shards:
        heights = jax.random.uniform(jax.random.fold_in(jax.random.fold_in(key, 6), position), (shards_of,), jnp.float32, low / len(shards), largest / len(shards))
        gain = gain * jnp.repeat(jnp.exp(heights), extent[position] // shards_of).reshape((-1,) + (1,) * (len(extent) - 1 - position))
    return gain


def rank_bounds(number_of, skew):
    portions = [(1 << 20) // math.isqrt(grade ** skew) + 1 for grade in range(1, number_of + 1)]
    width = 1 + sum(portions) // (1 << 30)
    return np.cumsum(np.array([max(1, weight // width) for weight in portions]))


def ranked_ids(rng, dims, count, skew):
    table = rank_bounds(count, skew)
    lot = jax.random.randint(jax.random.fold_in(rng, 1), dims, 0, int(table[count - 1]))
    standing = jnp.searchsorted(jnp.asarray(table, jnp.int32), lot, side="right")
    return jax.random.permutation(jax.random.fold_in(rng, 2), count)[standing].astype(jnp.int32)


def routed_block(own_key, own, number, rows, count, top, bound, lean):
    sequence = jax.random.permutation(own_key, count)
    heavy_load, common = portions_of(count, rows * top, bound, lean, True), portions_of(count, rows * top, bound, lean, False)
    places = jnp.arange(count)

    def named(lengths, rotation):
        used = int((lengths > 0).sum())
        fixed = max(1, used // 4)
        moved = fixed + (places - fixed + rotation * (used - fixed)) % max(1, count - fixed)
        return jnp.zeros((count,), jnp.int32).at[sequence[jnp.where(places < fixed, places, moved)]].set(jnp.asarray(lengths, jnp.int32))

    lengths = jnp.where(number % 4 == 0, named(heavy_load, number // 4), named(common, number - number // 4 - 1))
    mixed = jax.random.permutation(jax.random.fold_in(own, 3), count)
    giver, sink = mixed[0:count // 2 * 2:2], mixed[1:count // 2 * 2:2]
    room = jnp.minimum(lengths[giver] - 1, bound - lengths[sink]) // 2
    room = jnp.where((giver == sequence[0]) | (sink == sequence[0]) | (lengths[sink] == 0), 0, jnp.maximum(room, 0))
    moved = jax.random.randint(jax.random.fold_in(own, 4), (count // 2,), 0, 1 << 20) % (room + 1)
    lengths = lengths.at[giver].add(-moved).at[sink].add(moved)
    labels = jnp.searchsorted(jnp.cumsum(lengths), jnp.arange(rows * top), side="right").astype(jnp.int32)
    listing = labels.reshape(top, rows).T
    listing = listing[jax.random.permutation(jax.random.fold_in(own, 1), rows)]
    rotation = jax.random.randint(jax.random.fold_in(own, 2), (rows, 1), 0, top)
    return jnp.take_along_axis(listing, (jnp.arange(top)[None, :] + rotation) % top, axis=1)


def portions_of(amount, total, bound, slope, full):
    weights = [(1 << 20) // math.isqrt(rank ** slope) + 1 for rank in range(1, amount + 1)]
    largest = bound if full else min(bound, max(-(-total // amount), total * weights[0] // sum(weights)))
    least = 1 if total - largest >= amount - 1 else 0
    counts, surplus = [largest] + [least] * (amount - 1), total - largest - least * (amount - 1)
    while surplus > 0:
        movable = [i for i in range(1, amount) if counts[i] < largest] or [i for i in range(1, amount) if counts[i] < bound]
        whole, budget = sum([weights[i] for i in movable]), surplus
        for i in movable:
            addition = min(bound - counts[i], max(1, budget * weights[i] // whole), surplus)
            counts[i] = counts[i] + addition
            surplus = surplus - addition
    return np.array(counts)


def normal_values(own_key, dims, scale, bound, split=(), kind=jnp.bfloat16):
    factor_of = shard_levels(own_key, dims, split, -0.22, 0.18) if split else 1.0
    values = jax.random.normal(own_key, dims, jnp.float32) * scale * factor_of
    return jnp.minimum(jnp.maximum(values, -bound), bound).astype(kind)


def setup_inputs(seed: int = 0) -> dict:
    key_of = jax.random.split(jax.random.key(seed), 10)
    queries = draw_queries(jax.random.fold_in(key_of[9], 71), 0)
    gate_pre = normal_values(key_of[1], (TOKENS, XW), 1.5, 6.0, ((0, 64), (1, 4)))
    cotangent = draw_cotangent(jax.random.fold_in(key_of[9], 71), 0)
    store = normal_values(key_of[3], (ROWS, D), 1.0, 6.0, ((0, 64),))
    store_gain = jnp.clip(1.0 + 0.18 * jax.random.normal(key_of[4], (D,), jnp.float32), 0.1, 1.9)
    w_key = normal_values(key_of[5], (D, XW), D ** -0.5, 0.125, ((1, 4),))
    w_value = normal_values(key_of[6], (D, XW), D ** -0.5, 0.125, ((1, 4),))
    owners_keys = jax.random.split(jax.random.fold_in(key_of[7], 1), BLOCKS // BLK_DEV)
    owners_turns = jax.random.permutation(jax.random.fold_in(key_of[7], 3), BLOCKS // BLK_DEV)
    owners = jax.vmap(lambda own, number: routed_block(jax.random.fold_in(key_of[7], 2), own, number, BLK_DEV, N_ST, NPB, CAP, 2))(owners_keys, owners_turns).reshape((BLOCKS, NPB))
    slots = set_ends(ranked_ids(key_of[8], (BLOCKS, NPB), PASS_DEV, 2), jax.random.fold_in(key_of[8], 3), 0, PASS_DEV - 1).astype(jnp.int32)
    return {"queries": queries, "gate_pre": gate_pre, "cotangent": cotangent, "store": store, "store_gain": store_gain, "w_key": w_key, "w_value": w_value, "owners": owners, "slots": slots}


EPS = 1e-06

def reference(queries, gate_pre, cotangent, store, store_gain, w_key, w_value, owners, slots):
    store_rows = store.astype(jnp.float32)
    row_inverse = lax.rsqrt(lax.optimization_barrier(jnp.mean(store_rows * store_rows, axis=-1, keepdims=True)) + EPS)
    normed = (store_rows * row_inverse * store_gain).astype(jnp.bfloat16)
    key_table = jnp.dot(normed, w_key, preferred_element_type=jnp.float32).astype(jnp.bfloat16).reshape(PASSAGES, PLEN, XW)
    value_table = jnp.dot(normed, w_value, preferred_element_type=jnp.float32).astype(jnp.bfloat16).reshape(PASSAGES, PLEN, XW)
    passage_ids = (owners * PASS_DEV + slots).astype(jnp.int32)
    score_scale = HD ** (-0.5)

    def one_group(group):
        query_part, gate_part, cot_part, id_part = group
        flat_ids = id_part.reshape(-1).astype(jnp.int32)
        group_keys = key_table[flat_ids].reshape(BLK_DEV, NPB * PLEN, HEADS, HD).astype(jnp.float32)
        group_values = value_table[flat_ids].reshape(BLK_DEV, NPB * PLEN, HEADS, HD).astype(jnp.float32)
        query_wide = query_part.astype(jnp.float32)
        scores = jnp.einsum('bqhd,bkhd->bhqk', query_wide, group_keys) * score_scale
        shifted = scores - lax.optimization_barrier(jnp.max(scores, axis=-1, keepdims=True))
        weights = jnp.exp(shifted)
        weights = weights / lax.optimization_barrier(jnp.sum(weights, axis=-1, keepdims=True))
        weights_half = lax.optimization_barrier(weights.astype(jnp.bfloat16)).astype(jnp.float32)
        grad_in = jax.nn.sigmoid(gate_part.astype(jnp.float32)) * cot_part.astype(jnp.float32)
        grad_in = lax.optimization_barrier(grad_in.astype(jnp.bfloat16)).astype(jnp.float32)
        attended = jnp.einsum('bhqk,bkhd->bqhd', weights_half, group_values)
        row_delta = lax.optimization_barrier(jnp.sum(grad_in * attended, axis=-1))
        grad_weights = jnp.einsum('bqhd,bkhd->bhqk', grad_in, group_values)
        grad_scores = weights * (grad_weights - jnp.transpose(row_delta, (0, 2, 1))[..., None])
        grad_half = lax.optimization_barrier(grad_scores.astype(jnp.bfloat16)).astype(jnp.float32)
        grad_query = jnp.einsum('bhqk,bkhd->bqhd', grad_half, group_keys) * score_scale
        grad_key = jnp.einsum('bhqk,bqhd->bkhd', grad_half, query_wide) * score_scale
        grad_value = jnp.einsum('bhqk,bqhd->bkhd', weights_half, grad_in)
        return (grad_query.reshape(BLK_DEV * BLK, XW), grad_key.reshape(BLK_DEV * NPB, PLEN, XW), grad_value.reshape(BLK_DEV * NPB, PLEN, XW))
    groups = (queries.reshape(N_ST, BLK_DEV, BLK, HEADS, HD), gate_pre.reshape(N_ST, BLK_DEV, BLK, HEADS, HD), cotangent.reshape(N_ST, BLK_DEV, BLK, HEADS, HD), passage_ids.reshape(N_ST, BLK_DEV, NPB))
    grad_queries, slot_keys, slot_values = lax.map(one_group, groups)
    grad_queries = grad_queries.reshape(TOKENS, XW)
    every_id = passage_ids.reshape(-1)
    passage_keys = jnp.zeros((PASSAGES, PLEN, XW), jnp.float32).at[every_id].add(slot_keys.reshape(BLOCKS * NPB, PLEN, XW))
    passage_values = jnp.zeros((PASSAGES, PLEN, XW), jnp.float32).at[every_id].add(slot_values.reshape(BLOCKS * NPB, PLEN, XW))
    passage_keys = passage_keys.astype(jnp.bfloat16).reshape(ROWS, XW)
    passage_values = passage_values.astype(jnp.bfloat16).reshape(ROWS, XW)
    grad_normed = jnp.dot(passage_keys, w_key.T, preferred_element_type=jnp.float32) + jnp.dot(passage_values, w_value.T, preferred_element_type=jnp.float32)
    grad_w_value = jnp.dot(normed.T, passage_values, preferred_element_type=jnp.float32)
    unit_rows = store_rows * row_inverse
    grad_unit = grad_normed * store_gain
    grad_store = row_inverse * (grad_unit - unit_rows * lax.optimization_barrier(jnp.mean(grad_unit * unit_rows, axis=-1, keepdims=True)))
    return (grad_queries, grad_store, grad_w_value)
```

```python
import functools

import jax
import jax.numpy as jnp
from jax import lax
from jax.experimental import pallas as pl
from jax.experimental.pallas import tpu as pltpu
from jax.sharding import Mesh
from jax.sharding import PartitionSpec as P

HD = 128
PLEN = 64
ST = ("st_0", "st_1", "st_2")
ST_TP = ("st_0", "st_1", "st_2", "tp")
MESH = pl.DeviceIdType.MESH
EPS = 1e-06
BF = jnp.bfloat16
F32 = jnp.float32

NN = (((1,), (0,)), ((), ()))
NT = (((1,), (1,)), ((), ()))
TN = (((0,), (0,)), ((), ()))


def dot(a, b, dims=NN):
    return lax.dot_general(a, b, dims, preferred_element_type=F32)


def kernel(
    cfg,
    store_hbm,
    wk_hbm,
    wv_hbm,
    q_hbm,
    gate_hbm,
    cot_hbm,
    gain_ref,
    req_ref,
    pos_ref,
    inv_ref,
    dq_ref,
    gs_ref,
    gw_ref,
    store,
    normed,
    wk_all,
    wv_all,
    q,
    gate,
    gin,
    table,
    snd_a,
    snd_b,
    k_rcv,
    v_rcv,
    dv_rcv,
    dk_snd_0,
    dk_snd_1,
    dk_rcv_0,
    dk_rcv_1,
    wts,
    slot_a,
    run,
    pas_v,
    pas_k,
    own_v,
    own_k,
    gn,
    gw_full,
    gwc_rcv,
    gwy,
    gwy_rcv,
    gwz,
    gwz_rcv,
    asked_v,
    meta_v,
    meta_s,
    load_sem,
    self_sem,
    ssem,
    rsem,
):
    nz, ny, nc, nx, npass = cfg
    nst = nz * ny * nc
    dk_snd = (dk_snd_0, dk_snd_1)
    dk_rcv = (dk_rcv_0, dk_rcv_1)
    rows, width = store.shape
    heads = wk_all.shape[2] // HD
    blocks = q.shape[0] // 128
    per = pos_ref.shape[0] // blocks
    quarter = rows // nx
    z = lax.axis_index("st_0")
    y = lax.axis_index("st_1")
    c = lax.axis_index("st_2")
    x = lax.axis_index("tp")
    me = (z * ny + y) * nc + c
    WV, REQ, K, V, DV, DK, WK, XV, XK, GC, GY, GZ = 0, 1, 2, 3, 4, 5, 7, 8, 9, 11, 12, 13

    def st_peer(i):
        pz = lax.rem(z + i // (ny * nc), nz)
        py = lax.rem(y + lax.rem(i // nc, ny), ny)
        pc = lax.rem(c + lax.rem(i, nc), nc)
        return (pz, py, pc, x), (pz * ny + py) * nc + pc

    def x_peer(i):
        px = lax.rem(x + i, nx)
        return (z, y, c, px), px

    barrier = pltpu.get_barrier_semaphore()

    @pl.loop(1, nst)
    def _(i):
        pl.semaphore_signal(barrier, inc=1, device_id=st_peer(i)[0], device_id_type=MESH)

    @pl.loop(1, nx)
    def _(i):
        pl.semaphore_signal(barrier, inc=1, device_id=x_peer(i)[0], device_id_type=MESH)

    chunk = rows // 5
    loads = [
        pltpu.make_async_copy(
            store_hbm.at[pl.ds(i * chunk, chunk)], store.at[pl.ds(i * chunk, chunk)], load_sem.at[i]
        )
        for i in range(5)
    ]
    load_k = pltpu.make_async_copy(wk_hbm, wk_all.at[x], load_sem.at[5])
    load_v = pltpu.make_async_copy(wv_hbm, wv_all.at[x], load_sem.at[6])
    load_q = pltpu.make_async_copy(q_hbm, q, load_sem.at[7])
    load_g = pltpu.make_async_copy(gate_hbm, gate, load_sem.at[8])
    load_c = pltpu.make_async_copy(cot_hbm, gin, load_sem.at[9])
    load_k.start()
    for cp in loads:
        cp.start()
    load_v.start()
    load_q.start()
    load_g.start()
    load_c.start()
    pl.semaphore_wait(barrier, nst + nx - 2)

    def send_st(src, dst, k):
        @pl.loop(1, nst)
        def _(i):
            device, t = st_peer(i)
            pltpu.make_async_remote_copy(
                src_ref=src.at[t],
                dst_ref=dst.at[me],
                send_sem=ssem.at[k],
                recv_sem=rsem.at[k],
                device_id=device,
                device_id_type=MESH,
            ).start()

        own = pltpu.make_async_copy(src.at[me], dst.at[me], self_sem.at[k])
        own.start()
        return own

    def bulk_wait(buf, n, sem):
        part = buf.at[pl.ds(0, n)]
        pltpu.make_async_copy(part, part, sem).wait()

    own_req = send_st(req_ref, asked_v, REQ)

    load_k.wait()
    for i in range(5):
        loads[i].wait()

        @pl.loop(0, chunk // 64)
        def _(j):
            at = pl.ds(pl.multiple_of(i * chunk + j * 64, 64), 64)
            s = store[at, :].astype(F32)
            r = lax.rsqrt(jnp.mean(s * s, axis=-1, keepdims=True) + EPS)
            normed[at, :] = (s * r * gain_ref[...]).astype(BF)

        at = pl.ds(i * chunk, chunk)
        part = pl.ds(i * (chunk // PLEN), chunk // PLEN)
        keys = dot(normed[at, :], wk_all[x]).astype(BF)
        table[part] = keys.reshape(chunk // PLEN, PLEN, heads * HD)

    own_req.wait()
    bulk_wait(asked_v, nst - 1, rsem.at[REQ])
    asked = asked_v[...].reshape(nst, 128)
    lane = lax.broadcasted_iota(jnp.int32, (nst, 128), 1)
    row = lax.broadcasted_iota(jnp.int32, (nst, 128), 0)
    slot_col = jnp.where(asked < 0, npass, asked)
    key_col = slot_col * nst + row
    diag = lane == row
    key_row = jnp.sum(jnp.where(diag, key_col, 0), axis=0, keepdims=True)
    below = (lane < nst) & (key_row < key_col)
    rank = jnp.sum(below.astype(jnp.int32), axis=1, keepdims=True)
    order_row = jnp.sum(jnp.where(rank == lane, row, 0), axis=0, keepdims=True)
    sorted_row = jnp.sum(jnp.where(rank == lane, slot_col, 0), axis=0, keepdims=True)
    keep_row = jnp.sum(
        jnp.where((rank == lane - 1) & (slot_col == sorted_row), 1, 0), axis=0, keepdims=True
    )
    last_row = jnp.sum((slot_col <= lane).astype(jnp.int32), axis=0, keepdims=True) - 1
    count_row = jnp.sum((slot_col == lane).astype(jnp.int32), axis=0, keepdims=True)
    pick_row = jnp.sum(jnp.where(diag, jnp.maximum(asked, 0), 0), axis=0, keepdims=True)
    meta_v[0:1, :] = pick_row
    meta_v[1:2, :] = order_row
    meta_v[2:3, :] = keep_row
    meta_v[3:4, :] = jnp.maximum(last_row, 0)
    meta_v[4:5, :] = jnp.minimum(count_row, 1)
    to_s = pltpu.make_async_copy(meta_v, meta_s, load_sem.at[10])
    to_s.start()
    to_s.wait()

    def gather(src, dst):
        @pl.loop(0, nst)
        def _(t):
            dst[t] = src[meta_s[0, t]]

    gather(table, snd_a)
    own_k_copy = send_st(snd_a, k_rcv, K)

    load_v.wait()
    for i in range(5):
        at = pl.ds(i * chunk, chunk)
        part = pl.ds(i * (chunk // PLEN), chunk // PLEN)
        values = dot(normed[at, :], wv_all[x]).astype(BF)
        table[part] = values.reshape(chunk // PLEN, PLEN, heads * HD)
    gather(table, snd_b)
    own_v_copy = send_st(snd_b, v_rcv, V)

    for w_all, k in ((wk_all, WK), (wv_all, WV)):

        @pl.loop(1, nx)
        def _(i):
            device, _px = x_peer(i)
            pltpu.make_async_remote_copy(
                src_ref=w_all.at[x],
                dst_ref=w_all.at[x],
                send_sem=ssem.at[k],
                recv_sem=rsem.at[k],
                device_id=device,
                device_id_type=MESH,
            ).start()

    load_q.wait()
    load_g.wait()
    load_c.wait()

    @pl.loop(0, blocks)
    def _(b):
        at = pl.ds(pl.multiple_of(b * 128, 128), 128)
        opened = jax.nn.sigmoid(gate[at, :].astype(F32))
        gin[at, :] = (opened * gin[at, :].astype(F32)).astype(BF)

    scale = HD ** (-0.5)

    def passages(ref, b, h):
        parts = [ref[pos_ref[b * per + j], :, h * HD : (h + 1) * HD] for j in range(per)]
        return jnp.concatenate(parts, axis=0)

    own_k_copy.wait()
    bulk_wait(k_rcv, nst - 1, rsem.at[K])

    @pl.loop(0, blocks)
    def _(b):
        at = pl.ds(pl.multiple_of(b * 128, 128), 128)
        for h in range(heads):
            cols = slice(h * HD, (h + 1) * HD)
            kh = passages(k_rcv, b, h)
            s = dot(kh, q[at, cols], NT) * scale
            e = jnp.exp(s - jnp.max(s, axis=0, keepdims=True))
            w = e / jnp.sum(e, axis=0, keepdims=True)
            wts[b * heads + h] = w
            dv = dot(w.astype(BF), gin[at, cols]).astype(BF)
            for j in range(per):
                slot_a[b * per + j, :, cols] = dv[j * PLEN : (j + 1) * PLEN]

    bulk_wait(snd_a, nst - 1, ssem.at[K])

    @pl.loop(0, nst)
    def _(t):
        snd_a[t] = slot_a[inv_ref[t]]

    own_dv_copy = send_st(snd_a, dv_rcv, DV)

    own_v_copy.wait()
    bulk_wait(v_rcv, nst - 1, rsem.at[V])

    for h in range(heads):
        cols = slice(h * HD, (h + 1) * HD)

        @pl.loop(0, blocks)
        def _(b):
            at = pl.ds(pl.multiple_of(b * 128, 128), 128)
            kh = passages(k_rcv, b, h)
            vh = passages(v_rcv, b, h)
            gwt = dot(vh, gin[at, cols], NT)
            w = wts[b * heads + h]
            delta = jnp.sum(w.astype(BF).astype(F32) * gwt, axis=0, keepdims=True)
            gsc = (w * (gwt - delta)).astype(BF)
            dk = (dot(gsc, q[at, cols]) * scale).astype(BF)
            for j in range(per):
                slot_a[b * per + j, :, cols] = dk[j * PLEN : (j + 1) * PLEN]
            dq_ref[at, cols] = dot(gsc, kh, TN) * scale

        @pl.loop(0, nst)
        def _(t):
            dk_snd[h][t] = slot_a[inv_ref[t], :, cols]

        send_st(dk_snd[h], dk_rcv[h], DK + h)

    def owner_sum(rcv, cols, out):
        def step(i, acc):
            acc = acc * meta_s[2, i].astype(F32) + rcv[meta_s[1, i]].astype(F32)
            run[i, :, cols] = acc.astype(BF)
            return acc

        wide = cols.stop - cols.start
        lax.fori_loop(0, nst, step, jnp.zeros((PLEN, wide), F32))

        @pl.loop(0, npass)
        def _(p):
            got = run[meta_s[3, p], :, cols].astype(F32)
            some = meta_s[4, p].astype(F32)
            out[pl.ds(pl.multiple_of(p * PLEN, PLEN), PLEN), :] = (got * some).astype(BF)

    def send_x(src, dst, k):
        @pl.loop(1, nx)
        def _(i):
            device, px = x_peer(i)
            pltpu.make_async_remote_copy(
                src_ref=src.at[pl.ds(pl.multiple_of(px * quarter, 64), quarter)],
                dst_ref=dst.at[x],
                send_sem=ssem.at[k],
                recv_sem=rsem.at[k],
                device_id=device,
                device_id_type=MESH,
            ).start()

        own = pltpu.make_async_copy(
            src.at[pl.ds(pl.multiple_of(x * quarter, 64), quarter)], dst.at[x], self_sem.at[k]
        )
        own.start()
        return own

    own_dv_copy.wait()
    bulk_wait(dv_rcv, nst - 1, rsem.at[DV])
    owner_sum(dv_rcv, slice(0, heads * HD), pas_v)
    own_xv = send_x(pas_v, own_v, XV)

    tile = 256
    pv_t = pas_v[...].T

    @pl.loop(0, width // tile)
    def _(j):
        at = pl.multiple_of(j * tile, tile)
        part = dot(pv_t, normed[:, pl.ds(at, tile)]).T
        gw_full[pl.ds(j * (tile // gw_full.shape[1]), tile // gw_full.shape[1])] = part.reshape(
            tile // gw_full.shape[1], gw_full.shape[1], heads * HD
        )

    other = lax.rem(c + 1, nc)
    gw_by = gw_full.reshape(nz * ny, nc, gw_full.shape[1], heads * HD)
    to_core = pltpu.make_async_remote_copy(
        src_ref=gw_by.at[:, other],
        dst_ref=gwc_rcv,
        send_sem=ssem.at[GC],
        recv_sem=rsem.at[GC],
        device_id=(z, y, other, x),
        device_id_type=MESH,
    )
    to_core.start()

    bulk_wait(wk_all, nx - 1, rsem.at[WK])
    bulk_wait(wv_all, nx - 1, rsem.at[WV])
    own_xv.wait()
    bulk_wait(own_v, nx - 1, rsem.at[XV])

    @pl.loop(0, width // tile)
    def _(j):
        at = pl.ds(pl.multiple_of(j * tile, tile), tile)
        acc = dot(own_v[0], wv_all[0, at, :], NT)
        for s in range(1, nx):
            acc += dot(own_v[s], wv_all[s, at, :], NT)
        gn[:, at] = acc

    to_core.wait()

    @pl.loop(0, nz * ny)
    def _(i):
        zi, yi = i // ny, lax.rem(i, ny)
        gwy[yi, zi] = gw_full[i * nc + c] + gwc_rcv[i]

    @pl.loop(1, ny)
    def _(i):
        py = lax.rem(y + i, ny)
        pltpu.make_async_remote_copy(
            src_ref=gwy.at[py],
            dst_ref=gwy_rcv.at[i],
            send_sem=ssem.at[GY],
            recv_sem=rsem.at[GY],
            device_id=(z, py, c, x),
            device_id_type=MESH,
        ).start()

    bulk_wait(gwy, ny - 1, ssem.at[GY])
    bulk_wait(gwy_rcv, ny - 1, rsem.at[GY])

    @pl.loop(0, nz)
    def _(i):
        acc = gwy[y, i]
        for j in range(1, ny):
            acc += gwy_rcv[j, i]
        gwz[i] = acc

    @pl.loop(1, nz)
    def _(i):
        pz = lax.rem(z + i, nz)
        pltpu.make_async_remote_copy(
            src_ref=gwz.at[pz],
            dst_ref=gwz_rcv.at[i],
            send_sem=ssem.at[GZ],
            recv_sem=rsem.at[GZ],
            device_id=(pz, y, c, x),
            device_id_type=MESH,
        ).start()

    def keys_half(h):
        own = pltpu.make_async_copy(dk_snd[h].at[me], dk_rcv[h].at[me], self_sem.at[DK + h])
        own.wait()
        bulk_wait(dk_rcv[h], nst - 1, rsem.at[DK + h])
        owner_sum(dk_rcv[h], slice(0, HD), pas_k.at[h])
        own_x = send_x(pas_k.at[h], own_k.at[h], XK + h)
        own_x.wait()
        bulk_wait(own_k.at[h], nx - 1, rsem.at[XK + h])

        @pl.loop(0, width // tile)
        def _(j):
            at = pl.ds(pl.multiple_of(j * tile, tile), tile)
            acc = gn[:, at]
            for s in range(nx):
                acc += dot(own_k[h, s], wk_all[s, at, h * HD : (h + 1) * HD], NT)
            gn[:, at] = acc

    for h in range(heads):
        keys_half(h)
        if h == 0:
            bulk_wait(gwz, nz - 1, ssem.at[GZ])
            bulk_wait(gwz_rcv, nz - 1, rsem.at[GZ])
            acc = gwz[z]
            for j in range(1, nz):
                acc += gwz_rcv[j]
            gw_ref[...] = acc

    @pl.loop(0, quarter // 32)
    def _(j):
        at = pl.ds(pl.multiple_of(j * 32, 32), 32)
        s = store[pl.ds(pl.multiple_of(x * quarter + j * 32, 32), 32), :].astype(F32)
        r = lax.rsqrt(jnp.mean(s * s, axis=-1, keepdims=True) + EPS)
        u = s * r
        g = gn[at, :] * gain_ref[...]
        gs_ref[at, :] = r * (g - u * jnp.mean(g * u, axis=-1, keepdims=True))

    bulk_wait(asked_v, nst - 1, ssem.at[REQ])
    bulk_wait(snd_b, nst - 1, ssem.at[V])
    bulk_wait(snd_a, nst - 1, ssem.at[DV])
    for h in range(heads):
        bulk_wait(dk_snd[h], nst - 1, ssem.at[DK + h])
        bulk_wait(own_k.at[h], nx - 1, ssem.at[XK + h])
    bulk_wait(wk_all, nx - 1, ssem.at[WK])
    bulk_wait(wv_all, nx - 1, ssem.at[WV])
    bulk_wait(own_v, nx - 1, ssem.at[XV])


def local(dims, queries, gate_pre, cotangent, store, store_gain, w_key, w_value, owners, slots):
    nz, ny, nc, nx = dims
    nst = nz * ny * nc
    blocks, per = owners.shape
    rows, width = store.shape
    tokens, cols = queries.shape
    heads = cols // HD
    npass = rows // PLEN
    count = blocks * per
    quarter = rows // nx
    piece = width // nst
    flat = owners.reshape(count)
    hits = flat[:, None] == jnp.arange(nst, dtype=jnp.int32)[None, :]
    req = jnp.max(jnp.where(hits, slots.reshape(count)[:, None], -1), axis=0)
    inv = jnp.max(jnp.where(hits, jnp.arange(count, dtype=jnp.int32)[:, None], 0), axis=0)
    req = jnp.broadcast_to(req[:, None, None], (nst, 1, 128))
    anywhere = pl.BlockSpec(memory_space=pl.ANY)
    vmem = pl.BlockSpec(memory_space=pltpu.VMEM)
    smem = pl.BlockSpec(memory_space=pltpu.SMEM)
    per_peer = pltpu.VMEM((nst, PLEN, cols), BF)
    per_head = pltpu.VMEM((nst, PLEN, HD), BF)
    return pl.pallas_call(
        functools.partial(kernel, (nz, ny, nc, nx, npass)),
        out_shape=(
            jax.ShapeDtypeStruct((tokens, cols), F32),
            jax.ShapeDtypeStruct((quarter, width), F32),
            jax.ShapeDtypeStruct((piece, cols), F32),
        ),
        in_specs=[anywhere] * 6 + [vmem, vmem, smem, smem],
        out_specs=(vmem, vmem, vmem),
        scratch_shapes=[
            pltpu.VMEM((rows, width), BF),
            pltpu.VMEM((rows, width), BF),
            pltpu.VMEM((nx, width, cols), BF),
            pltpu.VMEM((nx, width, cols), BF),
            pltpu.VMEM((tokens, cols), BF),
            pltpu.VMEM((tokens, cols), BF),
            pltpu.VMEM((tokens, cols), BF),
            pltpu.VMEM((npass, PLEN, cols), BF),
            per_peer,
            per_peer,
            per_peer,
            per_peer,
            per_peer,
            per_head,
            per_head,
            per_head,
            per_head,
            pltpu.VMEM((blocks * heads, per * PLEN, 128), F32),
            pltpu.VMEM((count, PLEN, cols), BF),
            per_peer,
            pltpu.VMEM((rows, cols), BF),
            pltpu.VMEM((heads, rows, HD), BF),
            pltpu.VMEM((nx, quarter, cols), BF),
            pltpu.VMEM((heads, nx, quarter, HD), BF),
            pltpu.VMEM((quarter, width), F32),
            pltpu.VMEM((nst, piece, cols), F32),
            pltpu.VMEM((nz * ny, piece, cols), F32),
            pltpu.VMEM((ny, nz, piece, cols), F32),
            pltpu.VMEM((ny, nz, piece, cols), F32),
            pltpu.VMEM((nz, piece, cols), F32),
            pltpu.VMEM((nz, piece, cols), F32),
            pltpu.VMEM((nst, 1, 128), jnp.int32),
            pltpu.VMEM((8, 128), jnp.int32),
            pltpu.SMEM((8, 128), jnp.int32),
            pltpu.SemaphoreType.DMA((11,)),
            pltpu.SemaphoreType.DMA((14,)),
            pltpu.SemaphoreType.DMA((14,)),
            pltpu.SemaphoreType.DMA((14,)),
        ],
        compiler_params=pltpu.CompilerParams(
            collective_id=0, has_side_effects=True, vmem_limit_bytes=67_043_328
        ),
    )(
        store,
        w_key,
        w_value,
        queries,
        gate_pre,
        cotangent,
        store_gain.reshape(1, width),
        req,
        flat,
        inv,
    )


def solution(mesh):
    nx = mesh.shape["tp"]
    nst = mesh.shape["st"]
    nz, ny, nc = nst // 8, 4, 2
    torus = Mesh(mesh.devices.reshape(nz, ny, nc, nx), ST_TP)
    return jax.shard_map(
        functools.partial(local, (nz, ny, nc, nx)),
        mesh=torus,
        in_specs=(
            P(ST, "tp"),
            P(ST, "tp"),
            P(ST, "tp"),
            P(ST, None),
            P(),
            P(None, "tp"),
            P(None, "tp"),
            P(ST, None),
            P(ST, None),
        ),
        out_specs=(P(ST, "tp"), P(ST_TP, None), P(ST, "tp")),
        check_vma=False,
    )
```

```python
import functools

import jax
import jax.numpy as jnp
from jax import lax
from jax.experimental import pallas as pl
from jax.experimental.pallas import tpu as pltpu
from jax.sharding import Mesh
from jax.sharding import PartitionSpec as P

HD = 128
PLEN = 64
ST = ("st_0", "st_1", "st_2")
ST_TP = ("st_0", "st_1", "st_2", "tp")
MESH = pl.DeviceIdType.MESH
EPS = 1e-06
BF = jnp.bfloat16
F32 = jnp.float32

NN = (((1,), (0,)), ((), ()))
NT = (((1,), (1,)), ((), ()))
TN = (((0,), (0,)), ((), ()))


def dot(a, b, dims=NN):
    return lax.dot_general(a, b, dims, preferred_element_type=F32)


def kernel(
    cfg,
    store_hbm,
    wk_hbm,
    wv_hbm,
    q_hbm,
    gate_hbm,
    cot_hbm,
    gain_ref,
    owners_ref,
    slots_ref,
    dq_ref,
    gs_ref,
    gw_ref,
    store,
    normed,
    wk_all,
    wv_all,
    q,
    gate,
    gin,
    table,
    snd_a,
    snd_b,
    k_rcv,
    v_rcv,
    dv_rcv,
    dk_snd_0,
    dk_snd_1,
    dk_snd_2,
    dk_rcv_0,
    dk_rcv_1,
    dk_rcv_2,
    wts,
    slot_a,
    run,
    pas_v,
    pas_k_0,
    pas_k_1,
    pas_k_2,
    own_v,
    own_k_0,
    own_k_1,
    own_k_2,
    gn,
    gw_full,
    gwc_rcv,
    gwy,
    gwy_rcv,
    gwz,
    gwz_rcv,
    req_ref,
    asked_v,
    meta_v,
    meta_s,
    load_sem,
    self_sem,
    ssem,
    rsem,
):
    nz, ny, nc, nx, npass = cfg
    nst = nz * ny * nc
    dk_snd = (dk_snd_0, dk_snd_1, dk_snd_2)
    dk_rcv = (dk_rcv_0, dk_rcv_1, dk_rcv_2)
    pas_k = (pas_k_0, pas_k_1, pas_k_2)
    own_k = (own_k_0, own_k_1, own_k_2)
    rows, width = store.shape
    heads = wk_all.shape[2] // HD
    blocks, per = owners_ref.shape
    quarter = rows // nx
    z = lax.axis_index("st_0")
    y = lax.axis_index("st_1")
    c = lax.axis_index("st_2")
    x = lax.axis_index("tp")
    me = (z * ny + y) * nc + c
    REQ, K, V, DV, WK, WV, XV, GC, GY, GZ, DK, XK = 0, 1, 2, 3, 4, 5, 6, 7, 8, 9, 10, 13

    def st_peer(i):
        pz = lax.rem(z + i // (ny * nc), nz)
        py = lax.rem(y + lax.rem(i // nc, ny), ny)
        pc = lax.rem(c + lax.rem(i, nc), nc)
        return (pz, py, pc, x), (pz * ny + py) * nc + pc

    def x_peer(i):
        px = lax.rem(x + i, nx)
        return (z, y, c, px), px

    barrier = pltpu.get_barrier_semaphore()

    @pl.loop(1, nst)
    def _(i):
        pl.semaphore_signal(barrier, inc=1, device_id=st_peer(i)[0], device_id_type=MESH)

    @pl.loop(1, nx)
    def _(i):
        pl.semaphore_signal(barrier, inc=1, device_id=x_peer(i)[0], device_id_type=MESH)

    chunk = rows // 5
    loads = [
        pltpu.make_async_copy(
            store_hbm.at[pl.ds(i * chunk, chunk)], store.at[pl.ds(i * chunk, chunk)], load_sem.at[i]
        )
        for i in range(5)
    ]
    load_k = pltpu.make_async_copy(wk_hbm, wk_all.at[x], load_sem.at[5])
    load_v = pltpu.make_async_copy(wv_hbm, wv_all.at[x], load_sem.at[6])
    load_q = pltpu.make_async_copy(q_hbm, q, load_sem.at[7])
    load_g = pltpu.make_async_copy(gate_hbm, gate, load_sem.at[8])
    load_c = pltpu.make_async_copy(cot_hbm, gin, load_sem.at[9])
    load_k.start()
    for cp in loads:
        cp.start()
    load_v.start()
    load_q.start()
    load_g.start()
    load_c.start()

    def send_st(src, dst, k):
        @pl.loop(1, nst)
        def _(i):
            device, t = st_peer(i)
            pltpu.make_async_remote_copy(
                src_ref=src.at[t],
                dst_ref=dst.at[me],
                send_sem=ssem.at[k],
                recv_sem=rsem.at[k],
                device_id=device,
                device_id_type=MESH,
            ).start()

        own = pltpu.make_async_copy(src.at[me], dst.at[me], self_sem.at[k])
        own.start()
        return own

    def bulk_wait(buf, n, sem):
        part = buf.at[pl.ds(0, n)]
        pltpu.make_async_copy(part, part, sem).wait()

    lane = lax.broadcasted_iota(jnp.int32, (nst, 128), 1)
    row = lax.broadcasted_iota(jnp.int32, (nst, 128), 0)
    req = jnp.full((nst, 128), -1, jnp.int32)
    place_row = jnp.zeros((1, 128), jnp.int32)
    for b in range(blocks):
        for j in range(per):
            req = jnp.where(row == owners_ref[b, j], slots_ref[b, j], req)
            place_row = jnp.where(lane[0:1] == owners_ref[b, j], b * per + j, place_row)
    req_ref[...] = req.reshape(nst, 1, 128)
    meta_v[5:6, :] = place_row

    load_k.wait()
    for i in range(5):
        loads[i].wait()
        if i == 2:
            pl.semaphore_wait(barrier, nst + nx - 2)
            own_req = send_st(req_ref, asked_v, REQ)

        @pl.loop(0, chunk // 64)
        def _(j):
            at = pl.ds(pl.multiple_of(i * chunk + j * 64, 64), 64)
            s = store[at, :].astype(F32)
            r = lax.rsqrt(jnp.mean(s * s, axis=-1, keepdims=True) + EPS)
            normed[at, :] = (s * r * gain_ref[...]).astype(BF)

        at = pl.ds(i * chunk, chunk)
        part = pl.ds(i * (chunk // PLEN), chunk // PLEN)
        keys = dot(normed[at, :], wk_all[x]).astype(BF)
        table[part] = keys.reshape(chunk // PLEN, PLEN, heads * HD)

    own_req.wait()
    bulk_wait(asked_v, nst - 1, rsem.at[REQ])
    asked = asked_v[...].reshape(nst, 128)
    slot_col = jnp.where(asked < 0, npass, asked)
    key_col = slot_col * nst + row
    diag = lane == row
    key_row = jnp.sum(jnp.where(diag, key_col, 0), axis=0, keepdims=True)
    below = (lane < nst) & (key_row < key_col)
    rank = jnp.sum(below.astype(jnp.int32), axis=1, keepdims=True)
    order_row = jnp.sum(jnp.where(rank == lane, row, 0), axis=0, keepdims=True)
    sorted_row = jnp.sum(jnp.where(rank == lane, slot_col, 0), axis=0, keepdims=True)
    keep_row = jnp.sum(
        jnp.where((rank == lane - 1) & (slot_col == sorted_row), 1, 0), axis=0, keepdims=True
    )
    last_row = jnp.sum((slot_col <= lane).astype(jnp.int32), axis=0, keepdims=True) - 1
    count_row = jnp.sum((slot_col == lane).astype(jnp.int32), axis=0, keepdims=True)
    pick_row = jnp.sum(jnp.where(diag, jnp.maximum(asked, 0), 0), axis=0, keepdims=True)
    meta_v[0:1, :] = pick_row
    meta_v[1:2, :] = order_row
    meta_v[2:3, :] = keep_row
    meta_v[3:4, :] = jnp.maximum(last_row, 0)
    meta_v[4:5, :] = jnp.minimum(count_row, 1)
    to_s = pltpu.make_async_copy(meta_v, meta_s, load_sem.at[10])
    to_s.start()
    to_s.wait()

    def gather(src, dst):
        @pl.loop(0, nst)
        def _(t):
            dst[t] = src[meta_s[0, t]]

    gather(table, snd_a)
    own_k_copy = send_st(snd_a, k_rcv, K)

    load_v.wait()
    for i in range(5):
        at = pl.ds(i * chunk, chunk)
        part = pl.ds(i * (chunk // PLEN), chunk // PLEN)
        values = dot(normed[at, :], wv_all[x]).astype(BF)
        table[part] = values.reshape(chunk // PLEN, PLEN, heads * HD)
    gather(table, snd_b)
    own_v_copy = send_st(snd_b, v_rcv, V)

    for w_all, k in ((wk_all, WK), (wv_all, WV)):

        @pl.loop(1, nx)
        def _(i):
            device, _px = x_peer(i)
            pltpu.make_async_remote_copy(
                src_ref=w_all.at[x],
                dst_ref=w_all.at[x],
                send_sem=ssem.at[k],
                recv_sem=rsem.at[k],
                device_id=device,
                device_id_type=MESH,
            ).start()

    load_q.wait()
    load_g.wait()
    load_c.wait()

    @pl.loop(0, blocks)
    def _(b):
        at = pl.ds(pl.multiple_of(b * 128, 128), 128)
        opened = jax.nn.sigmoid(gate[at, :].astype(F32))
        gin[at, :] = (opened * gin[at, :].astype(F32)).astype(BF)

    scale = HD ** (-0.5)

    def passages(ref, b, h):
        parts = [ref[owners_ref[b, j], :, h * HD : (h + 1) * HD] for j in range(per)]
        return jnp.concatenate(parts, axis=0)

    own_k_copy.wait()
    bulk_wait(k_rcv, nst - 1, rsem.at[K])

    @pl.loop(0, blocks)
    def _(b):
        at = pl.ds(pl.multiple_of(b * 128, 128), 128)
        for h in range(heads):
            cols = slice(h * HD, (h + 1) * HD)
            kh = passages(k_rcv, b, h)
            s = dot(kh, q[at, cols], NT) * scale
            e = jnp.exp(s - jnp.max(s, axis=0, keepdims=True))
            w = e / jnp.sum(e, axis=0, keepdims=True)
            wts[b * heads + h] = w
            dv = dot(w.astype(BF), gin[at, cols]).astype(BF)
            for j in range(per):
                slot_a[b * per + j, :, cols] = dv[j * PLEN : (j + 1) * PLEN]

    bulk_wait(snd_a, nst - 1, ssem.at[K])

    @pl.loop(0, nst)
    def _(t):
        snd_a[t] = slot_a[meta_s[5, t]]

    own_dv_copy = send_st(snd_a, dv_rcv, DV)

    own_v_copy.wait()
    bulk_wait(v_rcv, nst - 1, rsem.at[V])

    @pl.loop(0, blocks)
    def _(b):
        at = pl.ds(pl.multiple_of(b * 128, 128), 128)
        for h in range(heads):
            cols = slice(h * HD, (h + 1) * HD)
            kh = passages(k_rcv, b, h)
            vh = passages(v_rcv, b, h)
            gwt = dot(vh, gin[at, cols], NT)
            w = wts[b * heads + h]
            delta = jnp.sum(w.astype(BF).astype(F32) * gwt, axis=0, keepdims=True)
            gsc = (w * (gwt - delta)).astype(BF)
            dk = (dot(gsc, q[at, cols]) * scale).astype(BF)
            for j in range(per):
                slot_a[b * per + j, :, cols] = dk[j * PLEN : (j + 1) * PLEN]
            dq_ref[at, cols] = (dot(gsc, kh, TN) * scale).astype(BF)

    half = PLEN // 2
    pieces = (
        (0, slice(0, heads * HD)),
        (1, slice(0, HD)),
        (1, slice(HD, heads * HD)),
    )

    def send_piece(k):
        part, cols = pieces[k]

        @pl.loop(0, nst)
        def _(t):
            dk_snd[k][t] = slot_a[meta_s[5, t], part * half : (part + 1) * half, cols]

        send_st(dk_snd[k], dk_rcv[k], DK + k)

    send_piece(0)

    def owner_sum(rcv, run, out):
        def step(i, acc):
            acc = acc * meta_s[2, i].astype(F32) + rcv[meta_s[1, i]].astype(F32)
            run[i] = acc.astype(BF)
            return acc

        lax.fori_loop(0, nst, step, jnp.zeros(rcv.shape[1:], F32))

        @pl.loop(0, npass)
        def _(p):
            got = run[meta_s[3, p]].astype(F32)
            out[p] = (got * meta_s[4, p].astype(F32)).astype(BF)

    few = npass // nx

    def send_x(src, dst, k):
        @pl.loop(1, nx)
        def _(i):
            device, px = x_peer(i)
            pltpu.make_async_remote_copy(
                src_ref=src.at[pl.ds(px * few, few)],
                dst_ref=dst.at[x],
                send_sem=ssem.at[k],
                recv_sem=rsem.at[k],
                device_id=device,
                device_id_type=MESH,
            ).start()

        own = pltpu.make_async_copy(src.at[pl.ds(x * few, few)], dst.at[x], self_sem.at[k])
        own.start()
        return own

    own_dv_copy.wait()
    bulk_wait(dv_rcv, nst - 1, rsem.at[DV])
    owner_sum(dv_rcv, run, pas_v)
    own_xv = send_x(pas_v, own_v, XV)

    tile = 256
    pv_t = pas_v[...].reshape(rows, heads * HD).T

    @pl.loop(0, width // tile)
    def _(j):
        at = pl.multiple_of(j * tile, tile)
        part = dot(pv_t, normed[:, pl.ds(at, tile)]).T
        gw_full[pl.ds(j * (tile // gw_full.shape[1]), tile // gw_full.shape[1])] = part.reshape(
            tile // gw_full.shape[1], gw_full.shape[1], heads * HD
        )

    other = lax.rem(c + 1, nc)
    gw_by = gw_full.reshape(nz * ny, nc, gw_full.shape[1], heads * HD)
    to_core = pltpu.make_async_remote_copy(
        src_ref=gw_by.at[:, other],
        dst_ref=gwc_rcv,
        send_sem=ssem.at[GC],
        recv_sem=rsem.at[GC],
        device_id=(z, y, other, x),
        device_id_type=MESH,
    )
    to_core.start()

    to_core.wait()

    @pl.loop(0, nz * ny)
    def _(i):
        zi, yi = i // ny, lax.rem(i, ny)
        gwy[yi, zi] = (gw_full[i * nc + c] + gwc_rcv[i]).astype(BF)

    @pl.loop(1, ny)
    def _(i):
        py = lax.rem(y + i, ny)
        pltpu.make_async_remote_copy(
            src_ref=gwy.at[py],
            dst_ref=gwy_rcv.at[i],
            send_sem=ssem.at[GY],
            recv_sem=rsem.at[GY],
            device_id=(z, py, c, x),
            device_id_type=MESH,
        ).start()

    send_piece(1)
    send_piece(2)

    bulk_wait(wk_all, nx - 1, rsem.at[WK])
    bulk_wait(wv_all, nx - 1, rsem.at[WV])
    own_xv.wait()
    bulk_wait(own_v, nx - 1, rsem.at[XV])

    @pl.loop(0, width // tile)
    def _(j):
        at = pl.ds(pl.multiple_of(j * tile, tile), tile)
        acc = dot(own_v[0].reshape(quarter, heads * HD), wv_all[0, at, :], NT)
        for s in range(1, nx):
            acc += dot(own_v[s].reshape(quarter, heads * HD), wv_all[s, at, :], NT)
        acc = acc.reshape(few, 2, half, tile)
        gn[0, :, at] = acc[:, 0].reshape(few * half, tile)
        gn[1, :, at] = acc[:, 1].reshape(few * half, tile)

    def keys_piece(k):
        part, cols = pieces[k]
        own = pltpu.make_async_copy(dk_snd[k].at[me], dk_rcv[k].at[me], self_sem.at[DK + k])
        own.wait()
        bulk_wait(dk_rcv[k], nst - 1, rsem.at[DK + k])
        bulk_wait(dk_snd[k], nst - 1, ssem.at[DK + k])
        owner_sum(dk_rcv[k], dk_snd[k], pas_k[k])
        own_x = send_x(pas_k[k], own_k[k], XK + k)
        own_x.wait()
        bulk_wait(own_k[k], nx - 1, rsem.at[XK + k])

        @pl.loop(0, width // tile)
        def _(j):
            at = pl.ds(pl.multiple_of(j * tile, tile), tile)
            acc = gn[part, :, at]
            for s in range(nx):
                mine = own_k[k][s].reshape(few * half, cols.stop - cols.start)
                acc += dot(mine, wk_all[s, at, cols], NT)
            gn[part, :, at] = acc

    def finish(part):
        @pl.loop(0, few)
        def _(j):
            at = pl.ds(pl.multiple_of(j * PLEN + part * half, half), half)
            first = x * quarter + j * PLEN + part * half
            s = store[pl.ds(pl.multiple_of(first, half), half), :].astype(F32)
            r = lax.rsqrt(jnp.mean(s * s, axis=-1, keepdims=True) + EPS)
            u = s * r
            g = gn[part, pl.ds(pl.multiple_of(j * half, half), half), :] * gain_ref[...]
            gs_ref[at, :] = (r * (g - u * jnp.mean(g * u, axis=-1, keepdims=True))).astype(BF)

    keys_piece(0)
    bulk_wait(gwy, ny - 1, ssem.at[GY])
    bulk_wait(gwy_rcv, ny - 1, rsem.at[GY])

    @pl.loop(0, nz)
    def _(i):
        acc = gwy[y, i].astype(F32)
        for j in range(1, ny):
            acc += gwy_rcv[j, i].astype(F32)
        gwz[i] = acc.astype(BF)

    @pl.loop(1, nz)
    def _(i):
        pz = lax.rem(z + i, nz)
        pltpu.make_async_remote_copy(
            src_ref=gwz.at[pz],
            dst_ref=gwz_rcv.at[i],
            send_sem=ssem.at[GZ],
            recv_sem=rsem.at[GZ],
            device_id=(pz, y, c, x),
            device_id_type=MESH,
        ).start()

    finish(0)
    keys_piece(1)
    keys_piece(2)
    finish(1)
    bulk_wait(gwz, nz - 1, ssem.at[GZ])
    bulk_wait(gwz_rcv, nz - 1, rsem.at[GZ])
    acc = gwz[z].astype(F32)
    for j in range(1, nz):
        acc += gwz_rcv[j].astype(F32)
    gw_ref[...] = acc

    bulk_wait(asked_v, nst - 1, ssem.at[REQ])
    bulk_wait(snd_b, nst - 1, ssem.at[V])
    bulk_wait(snd_a, nst - 1, ssem.at[DV])
    for k in range(3):
        bulk_wait(own_k[k], nx - 1, ssem.at[XK + k])
    bulk_wait(wk_all, nx - 1, ssem.at[WK])
    bulk_wait(wv_all, nx - 1, ssem.at[WV])
    bulk_wait(own_v, nx - 1, ssem.at[XV])


def local(dims, queries, gate_pre, cotangent, store, store_gain, w_key, w_value, owners, slots):
    nz, ny, nc, nx = dims
    nst = nz * ny * nc
    blocks, per = owners.shape
    rows, width = store.shape
    tokens, cols = queries.shape
    heads = cols // HD
    npass = rows // PLEN
    count = blocks * per
    quarter = rows // nx
    piece = width // nst
    anywhere = pl.BlockSpec(memory_space=pl.ANY)
    vmem = pl.BlockSpec(memory_space=pltpu.VMEM)
    smem = pl.BlockSpec(memory_space=pltpu.SMEM)
    per_peer = pltpu.VMEM((nst, PLEN, cols), BF)
    half = PLEN // 2
    few = npass // nx
    wide = pltpu.VMEM((nst, half, cols), BF)
    narrow = pltpu.VMEM((nst, half, HD), BF)
    dq, gs, gw = pl.pallas_call(
        functools.partial(kernel, (nz, ny, nc, nx, npass)),
        out_shape=(
            jax.ShapeDtypeStruct((tokens, cols), BF),
            jax.ShapeDtypeStruct((quarter, width), BF),
            jax.ShapeDtypeStruct((piece, cols), F32),
        ),
        in_specs=[anywhere] * 6 + [vmem, smem, smem],
        out_specs=(vmem, vmem, vmem),
        scratch_shapes=[
            pltpu.VMEM((rows, width), BF),
            pltpu.VMEM((rows, width), BF),
            pltpu.VMEM((nx, width, cols), BF),
            pltpu.VMEM((nx, width, cols), BF),
            pltpu.VMEM((tokens, cols), BF),
            pltpu.VMEM((tokens, cols), BF),
            pltpu.VMEM((tokens, cols), BF),
            pltpu.VMEM((npass, PLEN, cols), BF),
            per_peer,
            per_peer,
            per_peer,
            per_peer,
            per_peer,
            wide,
            narrow,
            narrow,
            wide,
            narrow,
            narrow,
            pltpu.VMEM((blocks * heads, per * PLEN, 128), F32),
            pltpu.VMEM((count, PLEN, cols), BF),
            per_peer,
            pltpu.VMEM((npass, PLEN, cols), BF),
            pltpu.VMEM((npass, half, cols), BF),
            pltpu.VMEM((npass, half, HD), BF),
            pltpu.VMEM((npass, half, HD), BF),
            pltpu.VMEM((nx, few, PLEN, cols), BF),
            pltpu.VMEM((nx, few, half, cols), BF),
            pltpu.VMEM((nx, few, half, HD), BF),
            pltpu.VMEM((nx, few, half, HD), BF),
            pltpu.VMEM((2, few * half, width), F32),
            pltpu.VMEM((nst, piece, cols), F32),
            pltpu.VMEM((nz * ny, piece, cols), F32),
            pltpu.VMEM((ny, nz, piece, cols), BF),
            pltpu.VMEM((ny, nz, piece, cols), BF),
            pltpu.VMEM((nz, piece, cols), BF),
            pltpu.VMEM((nz, piece, cols), BF),
            pltpu.VMEM((nst, 1, 128), jnp.int32),
            pltpu.VMEM((nst, 1, 128), jnp.int32),
            pltpu.VMEM((8, 128), jnp.int32),
            pltpu.SMEM((8, 128), jnp.int32),
            pltpu.SemaphoreType.DMA((11,)),
            pltpu.SemaphoreType.DMA((16,)),
            pltpu.SemaphoreType.DMA((16,)),
            pltpu.SemaphoreType.DMA((16,)),
        ],
        compiler_params=pltpu.CompilerParams(
            collective_id=0, has_side_effects=True, vmem_limit_bytes=67_043_328
        ),
    )(
        store,
        w_key,
        w_value,
        queries,
        gate_pre,
        cotangent,
        store_gain.reshape(1, width),
        owners,
        slots,
    )
    return dq.astype(F32), gs.astype(F32), gw


def solution(mesh):
    nx = mesh.shape["tp"]
    nst = mesh.shape["st"]
    nz, ny, nc = nst // 8, 4, 2
    torus = Mesh(mesh.devices.reshape(nz, ny, nc, nx), ST_TP)
    return jax.shard_map(
        functools.partial(local, (nz, ny, nc, nx)),
        mesh=torus,
        in_specs=(
            P(ST, "tp"),
            P(ST, "tp"),
            P(ST, "tp"),
            P(ST, None),
            P(),
            P(None, "tp"),
            P(None, "tp"),
            P(ST, None),
            P(ST, None),
        ),
        out_specs=(P(ST, "tp"), P(ST_TP, None), P(ST, "tp")),
        check_vma=False,
    )
```

```python
import functools

import jax
import jax.numpy as jnp
from jax import lax
from jax.experimental import pallas as pl
from jax.experimental.pallas import tpu as pltpu
from jax.sharding import Mesh
from jax.sharding import PartitionSpec as P

HD = 128
PLEN = 64
ST = ("st_0", "st_1", "st_2")
ST_TP = ("st_0", "st_1", "st_2", "tp")
MESH = pl.DeviceIdType.MESH
EPS = 1e-06
BF = jnp.bfloat16
F32 = jnp.float32

NN = (((1,), (0,)), ((), ()))
NT = (((1,), (1,)), ((), ()))
TN = (((0,), (0,)), ((), ()))


def dot(a, b, dims=NN):
    return lax.dot_general(a, b, dims, preferred_element_type=F32)


def kernel(
    cfg,
    store_hbm,
    wk_hbm,
    wv_hbm,
    q_hbm,
    gate_hbm,
    cot_hbm,
    gain_hbm,
    owners_hbm,
    slots_hbm,
    dq_ref,
    gs_ref,
    gw_ref,
    store,
    normed,
    wk_all,
    wv_all,
    q,
    gate,
    gin,
    table,
    snd_a,
    snd_b,
    k_rcv,
    v_rcv,
    dv_rcv,
    dk_snd_0,
    dk_snd_1,
    dk_snd_2,
    dk_rcv_0,
    dk_rcv_1,
    dk_rcv_2,
    wts,
    slot_a,
    run,
    pas_v,
    pas_k_0,
    pas_k_1,
    pas_k_2,
    own_v,
    own_k_0,
    own_k_1,
    own_k_2,
    gn,
    gw_full,
    gwc_rcv,
    gwy,
    gwy_rcv,
    gwz,
    gwz_rcv,
    req_ref,
    asked_v,
    meta_v,
    meta_s,
    gain_ref,
    owners_ref,
    slots_ref,
    load_sem,
    self_sem,
    ssem,
    rsem,
):
    nz, ny, nc, nx, npass = cfg
    nst = nz * ny * nc
    dk_snd = (dk_snd_0, dk_snd_1, dk_snd_2)
    dk_rcv = (dk_rcv_0, dk_rcv_1, dk_rcv_2)
    pas_k = (pas_k_0, pas_k_1, pas_k_2)
    own_k = (own_k_0, own_k_1, own_k_2)
    rows, width = store.shape
    heads = wk_all.shape[2] // HD
    per, blocks = owners_ref.shape
    quarter = rows // nx
    z = lax.axis_index("st_0")
    y = lax.axis_index("st_1")
    c = lax.axis_index("st_2")
    x = lax.axis_index("tp")
    me = (z * ny + y) * nc + c
    REQ, K, V, DV, WK, WV, XV, GC, GY, GZ, DK, XK = 0, 1, 2, 3, 4, 5, 6, 7, 8, 9, 10, 13

    def each_st(act):
        others = [
            (lax.rem(y + dy, ny), lax.rem(c + dc, nc)) for dy in range(ny) for dc in range(nc)
        ]

        @pl.loop(1, nz)
        def _(dz):
            pz = lax.rem(z + dz, nz)
            for py, pc in others:
                act((pz, py, pc, x), (pz * ny + py) * nc + pc)

        for py, pc in others[1:]:
            act((z, py, pc, x), (z * ny + py) * nc + pc)

    def x_peer(i):
        px = lax.rem(x + i, nx)
        return (z, y, c, px), px

    barrier = pltpu.get_barrier_semaphore()

    each_st(
        lambda device, t: pl.semaphore_signal(
            barrier, inc=1, device_id=device, device_id_type=MESH
        )
    )

    @pl.loop(1, nx)
    def _(i):
        pl.semaphore_signal(barrier, inc=1, device_id=x_peer(i)[0], device_id_type=MESH)

    chunk = rows // 5
    loads = [
        pltpu.make_async_copy(
            store_hbm.at[pl.ds(i * chunk, chunk)], store.at[pl.ds(i * chunk, chunk)], load_sem.at[i]
        )
        for i in range(5)
    ]
    load_k = pltpu.make_async_copy(wk_hbm, wk_all.at[x], load_sem.at[5])
    load_v = pltpu.make_async_copy(wv_hbm, wv_all.at[x], load_sem.at[6])
    load_q = pltpu.make_async_copy(q_hbm, q, load_sem.at[7])
    load_g = pltpu.make_async_copy(gate_hbm, gate, load_sem.at[8])
    load_c = pltpu.make_async_copy(cot_hbm, gin, load_sem.at[9])
    small = [
        pltpu.make_async_copy(src, dst, load_sem.at[11 + i])
        for i, (src, dst) in enumerate(
            ((owners_hbm, owners_ref), (slots_hbm, slots_ref), (gain_hbm, gain_ref))
        )
    ]
    for cp in small:
        cp.start()
    load_k.start()
    for cp in loads:
        cp.start()
    load_v.start()
    load_q.start()
    load_g.start()
    load_c.start()

    def send_st(src, dst, k):
        def start(device, t):
            pltpu.make_async_remote_copy(
                src_ref=src.at[t],
                dst_ref=dst.at[me],
                send_sem=ssem.at[k],
                recv_sem=rsem.at[k],
                device_id=device,
                device_id_type=MESH,
            ).start()

        each_st(start)
        own = pltpu.make_async_copy(src.at[me], dst.at[me], self_sem.at[k])
        own.start()
        return own

    def bulk_wait(buf, n, sem):
        part = buf.at[pl.ds(0, n)]
        pltpu.make_async_copy(part, part, sem).wait()

    lane = lax.broadcasted_iota(jnp.int32, (nst, 128), 1)
    row = lax.broadcasted_iota(jnp.int32, (nst, 128), 0)
    req = jnp.full((nst, 128), -1, jnp.int32)
    place_row = jnp.zeros((1, 128), jnp.int32)
    for cp in small:
        cp.wait()
    for b in range(blocks):
        for j in range(per):
            req = jnp.where(row == owners_ref[j, b], slots_ref[j, b], req)
            place_row = jnp.where(lane[0:1] == owners_ref[j, b], b * per + j, place_row)
    req_ref[...] = req.reshape(nst, 1, 128)
    meta_v[5:6, :] = place_row

    load_k.wait()
    for i in range(5):
        loads[i].wait()
        if i == 2:
            pl.semaphore_wait(barrier, nst + nx - 2)
            own_req = send_st(req_ref, asked_v, REQ)

        @pl.loop(0, chunk // 64)
        def _(j):
            at = pl.ds(pl.multiple_of(i * chunk + j * 64, 64), 64)
            s = store[at, :].astype(F32)
            r = lax.rsqrt(jnp.mean(s * s, axis=-1, keepdims=True) + EPS)
            normed[at, :] = (s * r * gain_ref[...]).astype(BF)

        at = pl.ds(i * chunk, chunk)
        part = pl.ds(i * (chunk // PLEN), chunk // PLEN)
        keys = dot(normed[at, :], wk_all[x]).astype(BF)
        table[part] = keys.reshape(chunk // PLEN, PLEN, heads * HD)

    own_req.wait()
    bulk_wait(asked_v, nst - 1, rsem.at[REQ])
    asked = asked_v[...].reshape(nst, 128)
    slot_col = jnp.where(asked < 0, npass, asked)
    key_col = slot_col * nst + row
    diag = lane == row
    key_row = jnp.sum(jnp.where(diag, key_col, 0), axis=0, keepdims=True)
    below = (lane < nst) & (key_row < key_col)
    rank = jnp.sum(below.astype(jnp.int32), axis=1, keepdims=True)
    order_row = jnp.sum(jnp.where(rank == lane, row, 0), axis=0, keepdims=True)
    sorted_row = jnp.sum(jnp.where(rank == lane, slot_col, 0), axis=0, keepdims=True)
    keep_row = jnp.sum(
        jnp.where((rank == lane - 1) & (slot_col == sorted_row), 1, 0), axis=0, keepdims=True
    )
    last_row = jnp.sum((slot_col <= lane).astype(jnp.int32), axis=0, keepdims=True) - 1
    count_row = jnp.sum((slot_col == lane).astype(jnp.int32), axis=0, keepdims=True)
    pick_row = jnp.sum(jnp.where(diag, jnp.maximum(asked, 0), 0), axis=0, keepdims=True)
    meta_v[0:1, :] = pick_row
    meta_v[1:2, :] = order_row
    meta_v[2:3, :] = keep_row
    meta_v[3:4, :] = jnp.maximum(last_row, 0)
    meta_v[4:5, :] = jnp.minimum(count_row, 1)
    to_s = pltpu.make_async_copy(meta_v, meta_s, load_sem.at[10])
    to_s.start()
    to_s.wait()

    def gather(src, dst):
        @pl.loop(0, nst)
        def _(t):
            dst[t] = src[meta_s[0, t]]

    gather(table, snd_a)
    own_k_copy = send_st(snd_a, k_rcv, K)

    load_v.wait()
    for i in range(5):
        at = pl.ds(i * chunk, chunk)
        part = pl.ds(i * (chunk // PLEN), chunk // PLEN)
        values = dot(normed[at, :], wv_all[x]).astype(BF)
        table[part] = values.reshape(chunk // PLEN, PLEN, heads * HD)
    gather(table, snd_b)
    own_v_copy = send_st(snd_b, v_rcv, V)

    for w_all, k in ((wk_all, WK), (wv_all, WV)):

        @pl.loop(1, nx)
        def _(i):
            device, _px = x_peer(i)
            pltpu.make_async_remote_copy(
                src_ref=w_all.at[x],
                dst_ref=w_all.at[x],
                send_sem=ssem.at[k],
                recv_sem=rsem.at[k],
                device_id=device,
                device_id_type=MESH,
            ).start()

    load_q.wait()
    load_g.wait()
    load_c.wait()

    @pl.loop(0, blocks)
    def _(b):
        at = pl.ds(pl.multiple_of(b * 128, 128), 128)
        opened = jax.nn.sigmoid(gate[at, :].astype(F32))
        gin[at, :] = (opened * gin[at, :].astype(F32)).astype(BF)

    scale = HD ** (-0.5)

    def passages(ref, b, h):
        parts = [ref[owners_ref[j, b], :, h * HD : (h + 1) * HD] for j in range(per)]
        return jnp.concatenate(parts, axis=0)

    own_k_copy.wait()
    bulk_wait(k_rcv, nst - 1, rsem.at[K])

    @pl.loop(0, blocks)
    def _(b):
        at = pl.ds(pl.multiple_of(b * 128, 128), 128)
        for h in range(heads):
            cols = slice(h * HD, (h + 1) * HD)
            kh = passages(k_rcv, b, h)
            s = dot(kh, q[at, cols], NT) * scale
            e = jnp.exp(s - jnp.max(s, axis=0, keepdims=True))
            w = e / jnp.sum(e, axis=0, keepdims=True)
            wts[b * heads + h] = w
            dv = dot(w.astype(BF), gin[at, cols]).astype(BF)
            for j in range(per):
                slot_a[b * per + j, :, cols] = dv[j * PLEN : (j + 1) * PLEN]

    bulk_wait(snd_a, nst - 1, ssem.at[K])

    @pl.loop(0, nst)
    def _(t):
        snd_a[t] = slot_a[meta_s[5, t]]

    own_dv_copy = send_st(snd_a, dv_rcv, DV)

    own_v_copy.wait()
    bulk_wait(v_rcv, nst - 1, rsem.at[V])

    @pl.loop(0, blocks)
    def _(b):
        at = pl.ds(pl.multiple_of(b * 128, 128), 128)
        for h in range(heads):
            cols = slice(h * HD, (h + 1) * HD)
            kh = passages(k_rcv, b, h)
            vh = passages(v_rcv, b, h)
            gwt = dot(vh, gin[at, cols], NT)
            w = wts[b * heads + h]
            delta = jnp.sum(w.astype(BF).astype(F32) * gwt, axis=0, keepdims=True)
            gsc = (w * (gwt - delta)).astype(BF)
            dk = (dot(gsc, q[at, cols]) * scale).astype(BF)
            for j in range(per):
                slot_a[b * per + j, :, cols] = dk[j * PLEN : (j + 1) * PLEN]
            dq_ref[at, cols] = (dot(gsc, kh, TN) * scale).astype(BF)

    half = PLEN // 2
    pieces = (
        (0, slice(0, heads * HD)),
        (1, slice(0, HD)),
        (1, slice(HD, heads * HD)),
    )

    def send_piece(k):
        part, cols = pieces[k]

        @pl.loop(0, nst)
        def _(t):
            dk_snd[k][t] = slot_a[meta_s[5, t], part * half : (part + 1) * half, cols]

        send_st(dk_snd[k], dk_rcv[k], DK + k)

    send_piece(0)

    def owner_sum(rcv, run, out):
        def step(i, acc):
            acc = acc * meta_s[2, i].astype(F32) + rcv[meta_s[1, i]].astype(F32)
            run[i] = acc.astype(BF)
            return acc

        lax.fori_loop(0, nst, step, jnp.zeros(rcv.shape[1:], F32))

        @pl.loop(0, npass)
        def _(p):
            got = run[meta_s[3, p]].astype(F32)
            out[p] = (got * meta_s[4, p].astype(F32)).astype(BF)

    few = npass // nx

    def send_x(src, dst, k):
        @pl.loop(1, nx)
        def _(i):
            device, px = x_peer(i)
            pltpu.make_async_remote_copy(
                src_ref=src.at[pl.ds(px * few, few)],
                dst_ref=dst.at[x],
                send_sem=ssem.at[k],
                recv_sem=rsem.at[k],
                device_id=device,
                device_id_type=MESH,
            ).start()

        own = pltpu.make_async_copy(src.at[pl.ds(x * few, few)], dst.at[x], self_sem.at[k])
        own.start()
        return own

    own_dv_copy.wait()
    bulk_wait(dv_rcv, nst - 1, rsem.at[DV])
    owner_sum(dv_rcv, run, pas_v)
    own_xv = send_x(pas_v, own_v, XV)

    tile = 256
    pv_t = pas_v[...].reshape(rows, heads * HD).T

    @pl.loop(0, width // tile)
    def _(j):
        at = pl.multiple_of(j * tile, tile)
        part = dot(pv_t, normed[:, pl.ds(at, tile)]).T
        gw_full[pl.ds(j * (tile // gw_full.shape[1]), tile // gw_full.shape[1])] = part.reshape(
            tile // gw_full.shape[1], gw_full.shape[1], heads * HD
        )

    other = lax.rem(c + 1, nc)
    gw_by = gw_full.reshape(nz * ny, nc, gw_full.shape[1], heads * HD)
    to_core = pltpu.make_async_remote_copy(
        src_ref=gw_by.at[:, other],
        dst_ref=gwc_rcv,
        send_sem=ssem.at[GC],
        recv_sem=rsem.at[GC],
        device_id=(z, y, other, x),
        device_id_type=MESH,
    )
    to_core.start()

    to_core.wait()

    @pl.loop(0, nz * ny)
    def _(i):
        zi, yi = i // ny, lax.rem(i, ny)
        gwy[yi, zi] = (gw_full[i * nc + c] + gwc_rcv[i]).astype(BF)

    @pl.loop(1, ny)
    def _(i):
        py = lax.rem(y + i, ny)
        pltpu.make_async_remote_copy(
            src_ref=gwy.at[py],
            dst_ref=gwy_rcv.at[i],
            send_sem=ssem.at[GY],
            recv_sem=rsem.at[GY],
            device_id=(z, py, c, x),
            device_id_type=MESH,
        ).start()

    send_piece(1)
    send_piece(2)

    bulk_wait(wk_all, nx - 1, rsem.at[WK])
    bulk_wait(wv_all, nx - 1, rsem.at[WV])
    own_xv.wait()
    bulk_wait(own_v, nx - 1, rsem.at[XV])

    @pl.loop(0, width // tile)
    def _(j):
        at = pl.ds(pl.multiple_of(j * tile, tile), tile)
        acc = dot(own_v[0].reshape(quarter, heads * HD), wv_all[0, at, :], NT)
        for s in range(1, nx):
            acc += dot(own_v[s].reshape(quarter, heads * HD), wv_all[s, at, :], NT)
        acc = acc.reshape(few, 2, half, tile)
        gn[0, :, at] = acc[:, 0].reshape(few * half, tile)
        gn[1, :, at] = acc[:, 1].reshape(few * half, tile)

    def keys_piece(k):
        part, cols = pieces[k]
        own = pltpu.make_async_copy(dk_snd[k].at[me], dk_rcv[k].at[me], self_sem.at[DK + k])
        own.wait()
        bulk_wait(dk_rcv[k], nst - 1, rsem.at[DK + k])
        bulk_wait(dk_snd[k], nst - 1, ssem.at[DK + k])
        owner_sum(dk_rcv[k], dk_snd[k], pas_k[k])
        own_x = send_x(pas_k[k], own_k[k], XK + k)
        own_x.wait()
        bulk_wait(own_k[k], nx - 1, rsem.at[XK + k])

        @pl.loop(0, width // tile)
        def _(j):
            at = pl.ds(pl.multiple_of(j * tile, tile), tile)
            acc = gn[part, :, at]
            for s in range(nx):
                mine = own_k[k][s].reshape(few * half, cols.stop - cols.start)
                acc += dot(mine, wk_all[s, at, cols], NT)
            gn[part, :, at] = acc

    def finish(part):
        @pl.loop(0, few)
        def _(j):
            at = pl.ds(pl.multiple_of(j * PLEN + part * half, half), half)
            first = x * quarter + j * PLEN + part * half
            s = store[pl.ds(pl.multiple_of(first, half), half), :].astype(F32)
            r = lax.rsqrt(jnp.mean(s * s, axis=-1, keepdims=True) + EPS)
            u = s * r
            g = gn[part, pl.ds(pl.multiple_of(j * half, half), half), :] * gain_ref[...]
            gs_ref[at, :] = (r * (g - u * jnp.mean(g * u, axis=-1, keepdims=True))).astype(BF)

    keys_piece(0)
    bulk_wait(gwy, ny - 1, ssem.at[GY])
    bulk_wait(gwy_rcv, ny - 1, rsem.at[GY])

    @pl.loop(0, nz)
    def _(i):
        acc = gwy[y, i].astype(F32)
        for j in range(1, ny):
            acc += gwy_rcv[j, i].astype(F32)
        gwz[i] = acc.astype(BF)

    @pl.loop(1, nz)
    def _(i):
        pz = lax.rem(z + i, nz)
        pltpu.make_async_remote_copy(
            src_ref=gwz.at[pz],
            dst_ref=gwz_rcv.at[i],
            send_sem=ssem.at[GZ],
            recv_sem=rsem.at[GZ],
            device_id=(pz, y, c, x),
            device_id_type=MESH,
        ).start()

    finish(0)
    keys_piece(1)
    keys_piece(2)
    finish(1)
    bulk_wait(gwz, nz - 1, ssem.at[GZ])
    bulk_wait(gwz_rcv, nz - 1, rsem.at[GZ])
    acc = gwz[z].astype(F32)
    for j in range(1, nz):
        acc += gwz_rcv[j].astype(F32)
    gw_ref[...] = acc

    bulk_wait(asked_v, nst - 1, ssem.at[REQ])
    bulk_wait(snd_b, nst - 1, ssem.at[V])
    bulk_wait(snd_a, nst - 1, ssem.at[DV])
    for k in range(3):
        bulk_wait(own_k[k], nx - 1, ssem.at[XK + k])
    bulk_wait(wk_all, nx - 1, ssem.at[WK])
    bulk_wait(wv_all, nx - 1, ssem.at[WV])
    bulk_wait(own_v, nx - 1, ssem.at[XV])


def local(dims, queries, gate_pre, cotangent, store, store_gain, w_key, w_value, owners, slots):
    nz, ny, nc, nx = dims
    nst = nz * ny * nc
    blocks, per = owners.shape
    rows, width = store.shape
    tokens, cols = queries.shape
    heads = cols // HD
    npass = rows // PLEN
    count = blocks * per
    quarter = rows // nx
    piece = width // nst
    anywhere = pl.BlockSpec(memory_space=pl.ANY)
    vmem = pl.BlockSpec(memory_space=pltpu.VMEM)
    per_peer = pltpu.VMEM((nst, PLEN, cols), BF)
    half = PLEN // 2
    few = npass // nx
    wide = pltpu.VMEM((nst, half, cols), BF)
    narrow = pltpu.VMEM((nst, half, HD), BF)
    dq, gs, gw = pl.pallas_call(
        functools.partial(kernel, (nz, ny, nc, nx, npass)),
        out_shape=(
            jax.ShapeDtypeStruct((tokens, cols), BF),
            jax.ShapeDtypeStruct((quarter, width), BF),
            jax.ShapeDtypeStruct((piece, cols), F32),
        ),
        in_specs=[anywhere] * 9,
        out_specs=(vmem, vmem, vmem),
        scratch_shapes=[
            pltpu.VMEM((rows, width), BF),
            pltpu.VMEM((rows, width), BF),
            pltpu.VMEM((nx, width, cols), BF),
            pltpu.VMEM((nx, width, cols), BF),
            pltpu.VMEM((tokens, cols), BF),
            pltpu.VMEM((tokens, cols), BF),
            pltpu.VMEM((tokens, cols), BF),
            pltpu.VMEM((npass, PLEN, cols), BF),
            per_peer,
            per_peer,
            per_peer,
            per_peer,
            per_peer,
            wide,
            narrow,
            narrow,
            wide,
            narrow,
            narrow,
            pltpu.VMEM((blocks * heads, per * PLEN, 128), F32),
            pltpu.VMEM((count, PLEN, cols), BF),
            per_peer,
            pltpu.VMEM((npass, PLEN, cols), BF),
            pltpu.VMEM((npass, half, cols), BF),
            pltpu.VMEM((npass, half, HD), BF),
            pltpu.VMEM((npass, half, HD), BF),
            pltpu.VMEM((nx, few, PLEN, cols), BF),
            pltpu.VMEM((nx, few, half, cols), BF),
            pltpu.VMEM((nx, few, half, HD), BF),
            pltpu.VMEM((nx, few, half, HD), BF),
            pltpu.VMEM((2, few * half, width), F32),
            pltpu.VMEM((nst, piece, cols), F32),
            pltpu.VMEM((nz * ny, piece, cols), F32),
            pltpu.VMEM((ny, nz, piece, cols), BF),
            pltpu.VMEM((ny, nz, piece, cols), BF),
            pltpu.VMEM((nz, piece, cols), BF),
            pltpu.VMEM((nz, piece, cols), BF),
            pltpu.VMEM((nst, 1, 128), jnp.int32),
            pltpu.VMEM((nst, 1, 128), jnp.int32),
            pltpu.VMEM((8, 128), jnp.int32),
            pltpu.SMEM((8, 128), jnp.int32),
            pltpu.VMEM((1, width), F32),
            pltpu.SMEM((per, blocks), jnp.int32),
            pltpu.SMEM((per, blocks), jnp.int32),
            pltpu.SemaphoreType.DMA((14,)),
            pltpu.SemaphoreType.DMA((16,)),
            pltpu.SemaphoreType.DMA((16,)),
            pltpu.SemaphoreType.DMA((16,)),
        ],
        compiler_params=pltpu.CompilerParams(
            collective_id=0, has_side_effects=True, vmem_limit_bytes=67_043_328
        ),
    )(
        store,
        w_key,
        w_value,
        queries,
        gate_pre,
        cotangent,
        store_gain.reshape(1, width),
        owners.T,
        slots.T,
    )
    return dq.astype(F32), gs.astype(F32), gw


def solution(mesh):
    nx = mesh.shape["tp"]
    nst = mesh.shape["st"]
    nz, ny, nc = nst // 8, 4, 2
    torus = Mesh(mesh.devices.reshape(nz, ny, nc, nx), ST_TP)
    return jax.shard_map(
        functools.partial(local, (nz, ny, nc, nx)),
        mesh=torus,
        in_specs=(
            P(ST, "tp"),
            P(ST, "tp"),
            P(ST, "tp"),
            P(ST, None),
            P(),
            P(None, "tp"),
            P(None, "tp"),
            P(ST, None),
            P(ST, None),
        ),
        out_specs=(P(ST, "tp"), P(ST_TP, None), P(ST, "tp")),
        check_vma=False,
    )
```

```python
import functools

import jax
import jax.numpy as jnp
from jax import lax
from jax.experimental import pallas as pl
from jax.experimental.pallas import tpu as pltpu
from jax.sharding import Mesh
from jax.sharding import PartitionSpec as P

HD = 128
PLEN = 64
ST = ("st_0", "st_1", "st_2")
ST_TP = ("st_0", "st_1", "st_2", "tp")
MESH = pl.DeviceIdType.MESH
EPS = 1e-06
BF = jnp.bfloat16
F32 = jnp.float32

NN = (((1,), (0,)), ((), ()))
NT = (((1,), (1,)), ((), ()))
TN = (((0,), (0,)), ((), ()))


def dot(a, b, dims=NN):
    return lax.dot_general(a, b, dims, preferred_element_type=F32)


def kernel(
    cfg,
    store_hbm,
    wk_hbm,
    wv_hbm,
    q_hbm,
    gate_hbm,
    cot_hbm,
    gain_hbm,
    owners_hbm,
    slots_hbm,
    dq_ref,
    gs_ref,
    gw_ref,
    store,
    normed,
    wk_all,
    wv_all,
    q,
    gate,
    gin,
    table,
    snd_a,
    snd_b,
    k_rcv,
    v_rcv,
    dv_rcv,
    dk_snd_0,
    dk_snd_1,
    dk_snd_2,
    dk_rcv_0,
    dk_rcv_1,
    dk_rcv_2,
    wts,
    slot_a,
    run,
    pas_v,
    pas_k_0,
    pas_k_1,
    pas_k_2,
    own_v,
    own_k_0,
    own_k_1,
    own_k_2,
    gn,
    gw_full,
    gwc_rcv,
    gwy,
    gwy_rcv,
    gwz,
    gwz_rcv,
    req_ref,
    asked_v,
    meta_v,
    meta_s,
    gain_ref,
    owners_ref,
    slots_ref,
    load_sem,
    self_sem,
    ssem,
    rsem,
):
    nz, ny, nc, nx, npass = cfg
    nst = nz * ny * nc
    dk_snd = (dk_snd_0, dk_snd_1, dk_snd_2)
    dk_rcv = (dk_rcv_0, dk_rcv_1, dk_rcv_2)
    pas_k = (pas_k_0, pas_k_1, pas_k_2)
    own_k = (own_k_0, own_k_1, own_k_2)
    rows, width = store.shape
    heads = wk_all.shape[2] // HD
    per, blocks = owners_ref.shape
    quarter = rows // nx
    z = lax.axis_index("st_0")
    y = lax.axis_index("st_1")
    c = lax.axis_index("st_2")
    x = lax.axis_index("tp")
    me = (z * ny + y) * nc + c
    REQ, K, V, DV, WK, WV, XV, GC, GY, GZ, DK, XK = 0, 1, 2, 3, 4, 5, 6, 7, 8, 9, 10, 13

    far_z = sorted(range(nz), key=lambda d: (-min(d, nz - d), d))
    far_y = sorted(range(ny), key=lambda d: (-min(d, ny - d), d))

    def each_st(act):
        def column(dy, dc, planes):
            py = lax.rem(y + dy, ny)
            pc = lax.rem(c + dc, nc)
            for dz in planes:
                pz = lax.rem(z + dz, nz)
                act((pz, py, pc, x), (pz * ny + py) * nc + pc)

        for dy in far_y[:-1]:

            @pl.loop(0, nc)
            def _(dc):
                column(dy, dc, far_z)

        column(0, 0, far_z[:-1])
        for dc in range(1, nc):
            column(0, dc, far_z)

    def x_peer(i):
        px = lax.rem(x + i, nx)
        return (z, y, c, px), px

    barrier = pltpu.get_barrier_semaphore()

    each_st(
        lambda device, t: pl.semaphore_signal(
            barrier, inc=1, device_id=device, device_id_type=MESH
        )
    )

    @pl.loop(1, nx)
    def _(i):
        pl.semaphore_signal(barrier, inc=1, device_id=x_peer(i)[0], device_id_type=MESH)

    chunk = rows // 5
    loads = [
        pltpu.make_async_copy(
            store_hbm.at[pl.ds(i * chunk, chunk)], store.at[pl.ds(i * chunk, chunk)], load_sem.at[i]
        )
        for i in range(5)
    ]
    load_k = pltpu.make_async_copy(wk_hbm, wk_all.at[x], load_sem.at[5])
    load_v = pltpu.make_async_copy(wv_hbm, wv_all.at[x], load_sem.at[6])
    load_q = pltpu.make_async_copy(q_hbm, q, load_sem.at[7])
    load_g = pltpu.make_async_copy(gate_hbm, gate, load_sem.at[8])
    load_c = pltpu.make_async_copy(cot_hbm, gin, load_sem.at[9])
    small = [
        pltpu.make_async_copy(src, dst, load_sem.at[11 + i])
        for i, (src, dst) in enumerate(
            ((owners_hbm, owners_ref), (slots_hbm, slots_ref), (gain_hbm, gain_ref))
        )
    ]
    for cp in small:
        cp.start()
    load_k.start()
    for cp in loads:
        cp.start()
    load_v.start()
    load_q.start()
    load_g.start()
    load_c.start()

    def send_st(src, dst, k):
        def start(device, t):
            pltpu.make_async_remote_copy(
                src_ref=src.at[t],
                dst_ref=dst.at[me],
                send_sem=ssem.at[k],
                recv_sem=rsem.at[k],
                device_id=device,
                device_id_type=MESH,
            ).start()

        each_st(start)
        own = pltpu.make_async_copy(src.at[me], dst.at[me], self_sem.at[k])
        own.start()
        return own

    def bulk_wait(buf, n, sem):
        part = buf.at[pl.ds(0, n)]
        pltpu.make_async_copy(part, part, sem).wait()

    lane = lax.broadcasted_iota(jnp.int32, (nst, 128), 1)
    row = lax.broadcasted_iota(jnp.int32, (nst, 128), 0)
    req = jnp.full((nst, 128), -1, jnp.int32)
    place_row = jnp.zeros((1, 128), jnp.int32)
    for cp in small:
        cp.wait()
    for b in range(blocks):
        for j in range(per):
            req = jnp.where(row == owners_ref[j, b], slots_ref[j, b], req)
            place_row = jnp.where(lane[0:1] == owners_ref[j, b], b * per + j, place_row)
    req_ref[...] = req.reshape(nst, 1, 128)
    meta_v[5:6, :] = place_row

    load_k.wait()
    for i in range(5):
        loads[i].wait()
        if i == 2:
            pl.semaphore_wait(barrier, nst + nx - 2)
            own_req = send_st(req_ref, asked_v, REQ)

        @pl.loop(0, chunk // 64)
        def _(j):
            at = pl.ds(pl.multiple_of(i * chunk + j * 64, 64), 64)
            s = store[at, :].astype(F32)
            r = lax.rsqrt(jnp.mean(s * s, axis=-1, keepdims=True) + EPS)
            normed[at, :] = (s * r * gain_ref[...]).astype(BF)

        at = pl.ds(i * chunk, chunk)
        part = pl.ds(i * (chunk // PLEN), chunk // PLEN)
        keys = dot(normed[at, :], wk_all[x]).astype(BF)
        table[part] = keys.reshape(chunk // PLEN, PLEN, heads * HD)

    own_req.wait()
    bulk_wait(asked_v, nst - 1, rsem.at[REQ])
    asked = asked_v[...].reshape(nst, 128)
    slot_col = jnp.where(asked < 0, npass, asked)
    key_col = slot_col * nst + row
    diag = lane == row
    key_row = jnp.sum(jnp.where(diag, key_col, 0), axis=0, keepdims=True)
    below = (lane < nst) & (key_row < key_col)
    rank = jnp.sum(below.astype(jnp.int32), axis=1, keepdims=True)
    order_row = jnp.sum(jnp.where(rank == lane, row, 0), axis=0, keepdims=True)
    sorted_row = jnp.sum(jnp.where(rank == lane, slot_col, 0), axis=0, keepdims=True)
    keep_row = jnp.sum(
        jnp.where((rank == lane - 1) & (slot_col == sorted_row), 1, 0), axis=0, keepdims=True
    )
    last_row = jnp.sum((slot_col <= lane).astype(jnp.int32), axis=0, keepdims=True) - 1
    count_row = jnp.sum((slot_col == lane).astype(jnp.int32), axis=0, keepdims=True)
    pick_row = jnp.sum(jnp.where(diag, jnp.maximum(asked, 0), 0), axis=0, keepdims=True)
    meta_v[0:1, :] = pick_row
    meta_v[1:2, :] = order_row
    meta_v[2:3, :] = keep_row
    meta_v[3:4, :] = jnp.maximum(last_row, 0)
    meta_v[4:5, :] = jnp.minimum(count_row, 1)
    to_s = pltpu.make_async_copy(meta_v, meta_s, load_sem.at[10])
    to_s.start()
    to_s.wait()

    def gather(src, dst):
        @pl.loop(0, nst)
        def _(t):
            dst[t] = src[meta_s[0, t]]

    gather(table, snd_a)
    own_k_copy = send_st(snd_a, k_rcv, K)

    load_v.wait()
    for i in range(5):
        at = pl.ds(i * chunk, chunk)
        part = pl.ds(i * (chunk // PLEN), chunk // PLEN)
        values = dot(normed[at, :], wv_all[x]).astype(BF)
        table[part] = values.reshape(chunk // PLEN, PLEN, heads * HD)
    gather(table, snd_b)
    own_v_copy = send_st(snd_b, v_rcv, V)

    for w_all, k in ((wk_all, WK), (wv_all, WV)):

        @pl.loop(1, nx)
        def _(i):
            device, _px = x_peer(i)
            pltpu.make_async_remote_copy(
                src_ref=w_all.at[x],
                dst_ref=w_all.at[x],
                send_sem=ssem.at[k],
                recv_sem=rsem.at[k],
                device_id=device,
                device_id_type=MESH,
            ).start()

    load_q.wait()
    load_g.wait()
    load_c.wait()

    @pl.loop(0, blocks)
    def _(b):
        at = pl.ds(pl.multiple_of(b * 128, 128), 128)
        opened = jax.nn.sigmoid(gate[at, :].astype(F32))
        gin[at, :] = (opened * gin[at, :].astype(F32)).astype(BF)

    scale = HD ** (-0.5)

    def passages(ref, b, h):
        parts = [ref[owners_ref[j, b], :, h * HD : (h + 1) * HD] for j in range(per)]
        return jnp.concatenate(parts, axis=0)

    own_k_copy.wait()
    bulk_wait(k_rcv, nst - 1, rsem.at[K])

    @pl.loop(0, blocks)
    def _(b):
        at = pl.ds(pl.multiple_of(b * 128, 128), 128)
        for h in range(heads):
            cols = slice(h * HD, (h + 1) * HD)
            kh = passages(k_rcv, b, h)
            s = dot(kh, q[at, cols], NT) * scale
            e = jnp.exp(s - jnp.max(s, axis=0, keepdims=True))
            w = e / jnp.sum(e, axis=0, keepdims=True)
            wts[b * heads + h] = w
            dv = dot(w.astype(BF), gin[at, cols]).astype(BF)
            for j in range(per):
                slot_a[b * per + j, :, cols] = dv[j * PLEN : (j + 1) * PLEN]

    bulk_wait(snd_a, nst - 1, ssem.at[K])

    @pl.loop(0, nst)
    def _(t):
        snd_a[t] = slot_a[meta_s[5, t]]

    own_dv_copy = send_st(snd_a, dv_rcv, DV)

    own_v_copy.wait()
    bulk_wait(v_rcv, nst - 1, rsem.at[V])

    @pl.loop(0, blocks)
    def _(b):
        at = pl.ds(pl.multiple_of(b * 128, 128), 128)
        for h in range(heads):
            cols = slice(h * HD, (h + 1) * HD)
            kh = passages(k_rcv, b, h)
            vh = passages(v_rcv, b, h)
            gwt = dot(vh, gin[at, cols], NT)
            w = wts[b * heads + h]
            delta = jnp.sum(w.astype(BF).astype(F32) * gwt, axis=0, keepdims=True)
            gsc = (w * (gwt - delta)).astype(BF)
            dk = (dot(gsc, q[at, cols]) * scale).astype(BF)
            for j in range(per):
                slot_a[b * per + j, :, cols] = dk[j * PLEN : (j + 1) * PLEN]
            dq_ref[at, cols] = (dot(gsc, kh, TN) * scale).astype(BF)

    half = PLEN // 2
    pieces = (
        (0, slice(0, heads * HD)),
        (1, slice(0, HD)),
        (1, slice(HD, heads * HD)),
    )

    def send_piece(k):
        part, cols = pieces[k]

        @pl.loop(0, nst)
        def _(t):
            dk_snd[k][t] = slot_a[meta_s[5, t], part * half : (part + 1) * half, cols]

        send_st(dk_snd[k], dk_rcv[k], DK + k)

    send_piece(0)

    def owner_sum(rcv, run, out):
        def step(i, acc):
            acc = acc * meta_s[2, i].astype(F32) + rcv[meta_s[1, i]].astype(F32)
            run[i] = acc.astype(BF)
            return acc

        lax.fori_loop(0, nst, step, jnp.zeros(rcv.shape[1:], F32))

        @pl.loop(0, npass)
        def _(p):
            got = run[meta_s[3, p]].astype(F32)
            out[p] = (got * meta_s[4, p].astype(F32)).astype(BF)

    few = npass // nx

    def send_x(src, dst, k):
        @pl.loop(1, nx)
        def _(i):
            device, px = x_peer(i)
            pltpu.make_async_remote_copy(
                src_ref=src.at[pl.ds(px * few, few)],
                dst_ref=dst.at[x],
                send_sem=ssem.at[k],
                recv_sem=rsem.at[k],
                device_id=device,
                device_id_type=MESH,
            ).start()

        own = pltpu.make_async_copy(src.at[pl.ds(x * few, few)], dst.at[x], self_sem.at[k])
        own.start()
        return own

    own_dv_copy.wait()
    bulk_wait(dv_rcv, nst - 1, rsem.at[DV])
    owner_sum(dv_rcv, run, pas_v)
    own_xv = send_x(pas_v, own_v, XV)

    tile = 256
    pv_t = pas_v[...].reshape(rows, heads * HD).T

    @pl.loop(0, width // tile)
    def _(j):
        at = pl.multiple_of(j * tile, tile)
        part = dot(pv_t, normed[:, pl.ds(at, tile)]).T
        gw_full[pl.ds(j * (tile // gw_full.shape[1]), tile // gw_full.shape[1])] = part.reshape(
            tile // gw_full.shape[1], gw_full.shape[1], heads * HD
        )

    other = lax.rem(c + 1, nc)
    gw_by = gw_full.reshape(nz * ny, nc, gw_full.shape[1], heads * HD)
    to_core = pltpu.make_async_remote_copy(
        src_ref=gw_by.at[:, other],
        dst_ref=gwc_rcv,
        send_sem=ssem.at[GC],
        recv_sem=rsem.at[GC],
        device_id=(z, y, other, x),
        device_id_type=MESH,
    )
    to_core.start()

    to_core.wait()

    @pl.loop(0, nz * ny)
    def _(i):
        zi, yi = i // ny, lax.rem(i, ny)
        gwy[yi, zi] = (gw_full[i * nc + c] + gwc_rcv[i]).astype(BF)

    @pl.loop(1, ny)
    def _(i):
        py = lax.rem(y + i, ny)
        pltpu.make_async_remote_copy(
            src_ref=gwy.at[py],
            dst_ref=gwy_rcv.at[i],
            send_sem=ssem.at[GY],
            recv_sem=rsem.at[GY],
            device_id=(z, py, c, x),
            device_id_type=MESH,
        ).start()

    send_piece(1)
    send_piece(2)

    bulk_wait(wk_all, nx - 1, rsem.at[WK])
    bulk_wait(wv_all, nx - 1, rsem.at[WV])
    own_xv.wait()
    bulk_wait(own_v, nx - 1, rsem.at[XV])

    @pl.loop(0, width // tile)
    def _(j):
        at = pl.ds(pl.multiple_of(j * tile, tile), tile)
        acc = dot(own_v[0].reshape(quarter, heads * HD), wv_all[0, at, :], NT)
        for s in range(1, nx):
            acc += dot(own_v[s].reshape(quarter, heads * HD), wv_all[s, at, :], NT)
        acc = acc.reshape(few, 2, half, tile)
        gn[0, :, at] = acc[:, 0].reshape(few * half, tile)
        gn[1, :, at] = acc[:, 1].reshape(few * half, tile)

    def keys_piece(k):
        part, cols = pieces[k]
        own = pltpu.make_async_copy(dk_snd[k].at[me], dk_rcv[k].at[me], self_sem.at[DK + k])
        own.wait()
        bulk_wait(dk_rcv[k], nst - 1, rsem.at[DK + k])
        bulk_wait(dk_snd[k], nst - 1, ssem.at[DK + k])
        owner_sum(dk_rcv[k], dk_snd[k], pas_k[k])
        own_x = send_x(pas_k[k], own_k[k], XK + k)
        own_x.wait()
        bulk_wait(own_k[k], nx - 1, rsem.at[XK + k])

        @pl.loop(0, width // tile)
        def _(j):
            at = pl.ds(pl.multiple_of(j * tile, tile), tile)
            acc = gn[part, :, at]
            for s in range(nx):
                mine = own_k[k][s].reshape(few * half, cols.stop - cols.start)
                acc += dot(mine, wk_all[s, at, cols], NT)
            gn[part, :, at] = acc

    def finish(part):
        @pl.loop(0, few)
        def _(j):
            at = pl.ds(pl.multiple_of(j * PLEN + part * half, half), half)
            first = x * quarter + j * PLEN + part * half
            s = store[pl.ds(pl.multiple_of(first, half), half), :].astype(F32)
            r = lax.rsqrt(jnp.mean(s * s, axis=-1, keepdims=True) + EPS)
            u = s * r
            g = gn[part, pl.ds(pl.multiple_of(j * half, half), half), :] * gain_ref[...]
            gs_ref[at, :] = (r * (g - u * jnp.mean(g * u, axis=-1, keepdims=True))).astype(BF)

    keys_piece(0)
    bulk_wait(gwy, ny - 1, ssem.at[GY])
    bulk_wait(gwy_rcv, ny - 1, rsem.at[GY])

    @pl.loop(0, nz)
    def _(i):
        acc = gwy[y, i].astype(F32)
        for j in range(1, ny):
            acc += gwy_rcv[j, i].astype(F32)
        gwz[i] = acc.astype(BF)

    @pl.loop(1, nz)
    def _(i):
        pz = lax.rem(z + i, nz)
        pltpu.make_async_remote_copy(
            src_ref=gwz.at[pz],
            dst_ref=gwz_rcv.at[i],
            send_sem=ssem.at[GZ],
            recv_sem=rsem.at[GZ],
            device_id=(pz, y, c, x),
            device_id_type=MESH,
        ).start()

    finish(0)
    keys_piece(1)
    keys_piece(2)
    finish(1)
    bulk_wait(gwz, nz - 1, ssem.at[GZ])
    bulk_wait(gwz_rcv, nz - 1, rsem.at[GZ])
    acc = gwz[z].astype(F32)
    for j in range(1, nz):
        acc += gwz_rcv[j].astype(F32)
    gw_ref[...] = acc

    bulk_wait(asked_v, nst - 1, ssem.at[REQ])
    bulk_wait(snd_b, nst - 1, ssem.at[V])
    bulk_wait(snd_a, nst - 1, ssem.at[DV])
    for k in range(3):
        bulk_wait(own_k[k], nx - 1, ssem.at[XK + k])
    bulk_wait(wk_all, nx - 1, ssem.at[WK])
    bulk_wait(wv_all, nx - 1, ssem.at[WV])
    bulk_wait(own_v, nx - 1, ssem.at[XV])


def local(dims, queries, gate_pre, cotangent, store, store_gain, w_key, w_value, owners, slots):
    nz, ny, nc, nx = dims
    nst = nz * ny * nc
    blocks, per = owners.shape
    rows, width = store.shape
    tokens, cols = queries.shape
    heads = cols // HD
    npass = rows // PLEN
    count = blocks * per
    quarter = rows // nx
    piece = width // nst
    anywhere = pl.BlockSpec(memory_space=pl.ANY)
    vmem = pl.BlockSpec(memory_space=pltpu.VMEM)
    per_peer = pltpu.VMEM((nst, PLEN, cols), BF)
    half = PLEN // 2
    few = npass // nx
    wide = pltpu.VMEM((nst, half, cols), BF)
    narrow = pltpu.VMEM((nst, half, HD), BF)
    dq, gs, gw = pl.pallas_call(
        functools.partial(kernel, (nz, ny, nc, nx, npass)),
        out_shape=(
            jax.ShapeDtypeStruct((tokens, cols), BF),
            jax.ShapeDtypeStruct((quarter, width), BF),
            jax.ShapeDtypeStruct((piece, cols), F32),
        ),
        in_specs=[anywhere] * 9,
        out_specs=(vmem, vmem, vmem),
        scratch_shapes=[
            pltpu.VMEM((rows, width), BF),
            pltpu.VMEM((rows, width), BF),
            pltpu.VMEM((nx, width, cols), BF),
            pltpu.VMEM((nx, width, cols), BF),
            pltpu.VMEM((tokens, cols), BF),
            pltpu.VMEM((tokens, cols), BF),
            pltpu.VMEM((tokens, cols), BF),
            pltpu.VMEM((npass, PLEN, cols), BF),
            per_peer,
            per_peer,
            per_peer,
            per_peer,
            per_peer,
            wide,
            narrow,
            narrow,
            wide,
            narrow,
            narrow,
            pltpu.VMEM((blocks * heads, per * PLEN, 128), F32),
            pltpu.VMEM((count, PLEN, cols), BF),
            per_peer,
            pltpu.VMEM((npass, PLEN, cols), BF),
            pltpu.VMEM((npass, half, cols), BF),
            pltpu.VMEM((npass, half, HD), BF),
            pltpu.VMEM((npass, half, HD), BF),
            pltpu.VMEM((nx, few, PLEN, cols), BF),
            pltpu.VMEM((nx, few, half, cols), BF),
            pltpu.VMEM((nx, few, half, HD), BF),
            pltpu.VMEM((nx, few, half, HD), BF),
            pltpu.VMEM((2, few * half, width), F32),
            pltpu.VMEM((nst, piece, cols), F32),
            pltpu.VMEM((nz * ny, piece, cols), F32),
            pltpu.VMEM((ny, nz, piece, cols), BF),
            pltpu.VMEM((ny, nz, piece, cols), BF),
            pltpu.VMEM((nz, piece, cols), BF),
            pltpu.VMEM((nz, piece, cols), BF),
            pltpu.VMEM((nst, 1, 128), jnp.int32),
            pltpu.VMEM((nst, 1, 128), jnp.int32),
            pltpu.VMEM((8, 128), jnp.int32),
            pltpu.SMEM((8, 128), jnp.int32),
            pltpu.VMEM((1, width), F32),
            pltpu.SMEM((per, blocks), jnp.int32),
            pltpu.SMEM((per, blocks), jnp.int32),
            pltpu.SemaphoreType.DMA((14,)),
            pltpu.SemaphoreType.DMA((16,)),
            pltpu.SemaphoreType.DMA((16,)),
            pltpu.SemaphoreType.DMA((16,)),
        ],
        compiler_params=pltpu.CompilerParams(
            collective_id=0, has_side_effects=True, vmem_limit_bytes=67_043_328
        ),
    )(
        store,
        w_key,
        w_value,
        queries,
        gate_pre,
        cotangent,
        store_gain.reshape(1, width),
        owners.T,
        slots.T,
    )
    return dq.astype(F32), gs.astype(F32), gw


def solution(mesh):
    nx = mesh.shape["tp"]
    nst = mesh.shape["st"]
    nz, ny, nc = nst // 8, 4, 2
    torus = Mesh(mesh.devices.reshape(nz, ny, nc, nx), ST_TP)
    return jax.shard_map(
        functools.partial(local, (nz, ny, nc, nx)),
        mesh=torus,
        in_specs=(
            P(ST, "tp"),
            P(ST, "tp"),
            P(ST, "tp"),
            P(ST, None),
            P(),
            P(None, "tp"),
            P(None, "tp"),
            P(ST, None),
            P(ST, None),
        ),
        out_specs=(P(ST, "tp"), P(ST_TP, None), P(ST, "tp")),
        check_vma=False,
    )
```

```python
import functools

import jax
import jax.numpy as jnp
from jax import lax
from jax.experimental import pallas as pl
from jax.experimental.pallas import tpu as pltpu
from jax.sharding import Mesh
from jax.sharding import PartitionSpec as P

HD = 128
PLEN = 64
ST = ("st_0", "st_1", "st_2")
ST_TP = ("st_0", "st_1", "st_2", "tp")
MESH = pl.DeviceIdType.MESH
EPS = 1e-06
BF = jnp.bfloat16
F32 = jnp.float32

NN = (((1,), (0,)), ((), ()))
NT = (((1,), (1,)), ((), ()))
TN = (((0,), (0,)), ((), ()))


def dot(a, b, dims=NN):
    return lax.dot_general(a, b, dims, preferred_element_type=F32)


def kernel(
    cfg,
    store_hbm,
    wk_hbm,
    wv_hbm,
    q_hbm,
    gate_hbm,
    cot_hbm,
    gain_hbm,
    owners_hbm,
    slots_hbm,
    dq_ref,
    gs_ref,
    gw_ref,
    store,
    normed,
    wk_all,
    wv_all,
    q,
    gate,
    gin,
    table,
    snd_a,
    snd_b,
    k_rcv,
    v_rcv,
    dv_rcv,
    dk_snd_0,
    dk_snd_1,
    dk_snd_2,
    dk_rcv_0,
    dk_rcv_1,
    dk_rcv_2,
    wts,
    slot_a,
    run,
    pas_v,
    pas_k_0,
    pas_k_1,
    pas_k_2,
    own_v,
    own_k_0,
    own_k_1,
    own_k_2,
    gn,
    gw_full,
    gwc_rcv,
    gwy,
    gwy_rcv,
    gwz,
    gwz_rcv,
    req_ref,
    asked_v,
    meta_v,
    meta_s,
    gain_ref,
    owners_ref,
    slots_ref,
    load_sem,
    self_sem,
    ssem,
    rsem,
):
    nz, ny, nc, nx, npass = cfg
    nst = nz * ny * nc
    dk_snd = (dk_snd_0, dk_snd_1, dk_snd_2)
    dk_rcv = (dk_rcv_0, dk_rcv_1, dk_rcv_2)
    pas_k = (pas_k_0, pas_k_1, pas_k_2)
    own_k = (own_k_0, own_k_1, own_k_2)
    rows, width = store.shape
    heads = wk_all.shape[2] // HD
    per, blocks = owners_ref.shape
    quarter = rows // nx
    z = lax.axis_index("st_0")
    y = lax.axis_index("st_1")
    c = lax.axis_index("st_2")
    x = lax.axis_index("tp")
    me = (z * ny + y) * nc + c
    REQ, K, V, DV, WK, WV, XV, GC, GY, GZ, DK, XK = 0, 1, 2, 3, 4, 5, 6, 7, 8, 9, 10, 13

    far_z = sorted(range(nz), key=lambda d: (-min(d, nz - d), d))
    far_y = sorted(range(ny), key=lambda d: (-min(d, ny - d), d))

    def each_st(act):
        def column(dy, dc, planes):
            py = lax.rem(y + dy, ny)
            pc = lax.rem(c + dc, nc)
            for dz in planes:
                pz = lax.rem(z + dz, nz)
                act((pz, py, pc, x), (pz * ny + py) * nc + pc)

        for dy in far_y[:-1]:

            @pl.loop(0, nc)
            def _(dc):
                column(dy, dc, far_z)

        column(0, 0, far_z[:-1])
        for dc in range(1, nc):
            column(0, dc, far_z)

    def x_peer(i):
        px = lax.rem(x + i, nx)
        return (z, y, c, px), px

    barrier = pltpu.get_barrier_semaphore()

    each_st(
        lambda device, t: pl.semaphore_signal(
            barrier, inc=1, device_id=device, device_id_type=MESH
        )
    )

    @pl.loop(1, nx)
    def _(i):
        pl.semaphore_signal(barrier, inc=1, device_id=x_peer(i)[0], device_id_type=MESH)

    chunk = rows // 5
    loads = [
        pltpu.make_async_copy(
            store_hbm.at[pl.ds(i * chunk, chunk)], store.at[pl.ds(i * chunk, chunk)], load_sem.at[i]
        )
        for i in range(5)
    ]
    load_k = pltpu.make_async_copy(wk_hbm, wk_all.at[x], load_sem.at[5])
    load_v = pltpu.make_async_copy(wv_hbm, wv_all.at[x], load_sem.at[6])
    load_q = pltpu.make_async_copy(q_hbm, q, load_sem.at[7])
    load_g = pltpu.make_async_copy(gate_hbm, gate, load_sem.at[8])
    load_c = pltpu.make_async_copy(cot_hbm, gin, load_sem.at[9])
    small = [
        pltpu.make_async_copy(src, dst, load_sem.at[11 + i])
        for i, (src, dst) in enumerate(
            ((owners_hbm, owners_ref), (slots_hbm, slots_ref), (gain_hbm, gain_ref))
        )
    ]
    for cp in small:
        cp.start()
    load_k.start()
    for cp in loads:
        cp.start()
    load_v.start()
    load_q.start()
    load_g.start()
    load_c.start()

    def send_st(src, dst, k):
        def start(device, t):
            pltpu.make_async_remote_copy(
                src_ref=src.at[t],
                dst_ref=dst.at[me],
                send_sem=ssem.at[k],
                recv_sem=rsem.at[k],
                device_id=device,
                device_id_type=MESH,
            ).start()

        each_st(start)
        own = pltpu.make_async_copy(src.at[me], dst.at[me], self_sem.at[k])
        own.start()
        return own

    def bulk_wait(buf, n, sem):
        part = buf.at[pl.ds(0, n)]
        pltpu.make_async_copy(part, part, sem).wait()

    lane = lax.broadcasted_iota(jnp.int32, (nst, 128), 1)
    row = lax.broadcasted_iota(jnp.int32, (nst, 128), 0)
    req = jnp.full((nst, 128), -1, jnp.int32)
    place_row = jnp.zeros((1, 128), jnp.int32)
    for cp in small:
        cp.wait()
    for b in range(blocks):
        for j in range(per):
            req = jnp.where(row == owners_ref[j, b], slots_ref[j, b], req)
            place_row = jnp.where(lane[0:1] == owners_ref[j, b], b * per + j, place_row)
    req_ref[...] = req.reshape(nst, 1, 128)
    meta_v[5:6, :] = place_row

    load_k.wait()
    for i in range(5):
        loads[i].wait()
        if i == 2:
            pl.semaphore_wait(barrier, nst + nx - 2)
            own_req = send_st(req_ref, asked_v, REQ)

        @pl.loop(0, chunk // 64)
        def _(j):
            at = pl.ds(pl.multiple_of(i * chunk + j * 64, 64), 64)
            s = store[at, :].astype(F32)
            r = lax.rsqrt(jnp.mean(s * s, axis=-1, keepdims=True) + EPS)
            normed[at, :] = (s * r * gain_ref[...]).astype(BF)

        at = pl.ds(i * chunk, chunk)
        part = pl.ds(i * (chunk // PLEN), chunk // PLEN)
        keys = dot(normed[at, :], wk_all[x]).astype(BF)
        table[part] = keys.reshape(chunk // PLEN, PLEN, heads * HD)

    own_req.wait()
    bulk_wait(asked_v, nst - 1, rsem.at[REQ])
    asked = asked_v[...].reshape(nst, 128)
    slot_col = jnp.where(asked < 0, npass, asked)
    key_col = slot_col * nst + row
    diag = lane == row
    key_row = jnp.sum(jnp.where(diag, key_col, 0), axis=0, keepdims=True)
    below = (lane < nst) & (key_row < key_col)
    rank = jnp.sum(below.astype(jnp.int32), axis=1, keepdims=True)
    order_row = jnp.sum(jnp.where(rank == lane, row, 0), axis=0, keepdims=True)
    sorted_row = jnp.sum(jnp.where(rank == lane, slot_col, 0), axis=0, keepdims=True)
    keep_row = jnp.sum(
        jnp.where((rank == lane - 1) & (slot_col == sorted_row), 1, 0), axis=0, keepdims=True
    )
    last_row = jnp.sum((slot_col <= lane).astype(jnp.int32), axis=0, keepdims=True) - 1
    count_row = jnp.sum((slot_col == lane).astype(jnp.int32), axis=0, keepdims=True)
    pick_row = jnp.sum(jnp.where(diag, jnp.maximum(asked, 0), 0), axis=0, keepdims=True)
    meta_v[0:1, :] = pick_row
    meta_v[1:2, :] = order_row
    meta_v[2:3, :] = keep_row
    meta_v[3:4, :] = jnp.maximum(last_row, 0)
    meta_v[4:5, :] = jnp.minimum(count_row, 1)
    to_s = pltpu.make_async_copy(meta_v, meta_s, load_sem.at[10])
    to_s.start()
    to_s.wait()

    def gather(src, dst):
        @pl.loop(0, nst)
        def _(t):
            dst[t] = src[meta_s[0, t]]

    gather(table, snd_a)
    own_k_copy = send_st(snd_a, k_rcv, K)

    load_v.wait()
    for i in range(5):
        at = pl.ds(i * chunk, chunk)
        part = pl.ds(i * (chunk // PLEN), chunk // PLEN)
        values = dot(normed[at, :], wv_all[x]).astype(BF)
        table[part] = values.reshape(chunk // PLEN, PLEN, heads * HD)
    gather(table, snd_b)
    own_v_copy = send_st(snd_b, v_rcv, V)

    for w_all, k in ((wk_all, WK), (wv_all, WV)):

        @pl.loop(1, nx)
        def _(i):
            device, _px = x_peer(i)
            pltpu.make_async_remote_copy(
                src_ref=w_all.at[x],
                dst_ref=w_all.at[x],
                send_sem=ssem.at[k],
                recv_sem=rsem.at[k],
                device_id=device,
                device_id_type=MESH,
            ).start()

    load_q.wait()
    load_g.wait()
    load_c.wait()

    @pl.loop(0, blocks)
    def _(b):
        at = pl.ds(pl.multiple_of(b * 128, 128), 128)
        opened = jax.nn.sigmoid(gate[at, :].astype(F32))
        gin[at, :] = (opened * gin[at, :].astype(F32)).astype(BF)

    scale = HD ** (-0.5)

    def passages(ref, b, h):
        parts = [ref[owners_ref[j, b], :, h * HD : (h + 1) * HD] for j in range(per)]
        return jnp.concatenate(parts, axis=0)

    own_k_copy.wait()
    bulk_wait(k_rcv, nst - 1, rsem.at[K])

    @pl.loop(0, blocks)
    def _(b):
        at = pl.ds(pl.multiple_of(b * 128, 128), 128)
        for h in range(heads):
            cols = slice(h * HD, (h + 1) * HD)
            kh = passages(k_rcv, b, h)
            s = dot(kh, q[at, cols], NT) * scale
            e = jnp.exp(s - jnp.max(s, axis=0, keepdims=True))
            w = e / jnp.sum(e, axis=0, keepdims=True)
            wts[b * heads + h] = w
            dv = dot(w.astype(BF), gin[at, cols]).astype(BF)
            for j in range(per):
                slot_a[b * per + j, :, cols] = dv[j * PLEN : (j + 1) * PLEN]

    bulk_wait(snd_a, nst - 1, ssem.at[K])

    @pl.loop(0, nst)
    def _(t):
        snd_a[t] = slot_a[meta_s[5, t]]

    own_dv_copy = send_st(snd_a, dv_rcv, DV)

    own_v_copy.wait()
    bulk_wait(v_rcv, nst - 1, rsem.at[V])

    @pl.loop(0, blocks)
    def _(b):
        at = pl.ds(pl.multiple_of(b * 128, 128), 128)
        for h in range(heads):
            cols = slice(h * HD, (h + 1) * HD)
            kh = passages(k_rcv, b, h)
            vh = passages(v_rcv, b, h)
            gwt = dot(vh, gin[at, cols], NT)
            w = wts[b * heads + h]
            delta = jnp.sum(w.astype(BF).astype(F32) * gwt, axis=0, keepdims=True)
            gsc = (w * (gwt - delta)).astype(BF)
            dk = (dot(gsc, q[at, cols]) * scale).astype(BF)
            for j in range(per):
                slot_a[b * per + j, :, cols] = dk[j * PLEN : (j + 1) * PLEN]
            dq_ref[at, cols] = (dot(gsc, kh, TN) * scale).astype(BF)

    half = PLEN // 2
    pieces = (
        (0, slice(0, heads * HD)),
        (1, slice(0, HD)),
        (1, slice(HD, heads * HD)),
    )

    def send_piece(k):
        part, cols = pieces[k]

        @pl.loop(0, nst)
        def _(t):
            dk_snd[k][t] = slot_a[meta_s[5, t], part * half : (part + 1) * half, cols]

        send_st(dk_snd[k], dk_rcv[k], DK + k)

    send_piece(0)

    def owner_sum(rcv, run, out):
        def step(i, acc):
            acc = acc * meta_s[2, i].astype(F32) + rcv[meta_s[1, i]].astype(F32)
            run[i] = acc.astype(BF)
            return acc

        lax.fori_loop(0, nst, step, jnp.zeros(rcv.shape[1:], F32))

        @pl.loop(0, npass)
        def _(p):
            got = run[meta_s[3, p]].astype(F32)
            out[p] = (got * meta_s[4, p].astype(F32)).astype(BF)

    few = npass // nx

    def send_x(src, dst, k):
        @pl.loop(1, nx)
        def _(i):
            device, px = x_peer(i)
            pltpu.make_async_remote_copy(
                src_ref=src.at[pl.ds(px * few, few)],
                dst_ref=dst.at[x],
                send_sem=ssem.at[k],
                recv_sem=rsem.at[k],
                device_id=device,
                device_id_type=MESH,
            ).start()

        own = pltpu.make_async_copy(src.at[pl.ds(x * few, few)], dst.at[x], self_sem.at[k])
        own.start()
        return own

    own_dv_copy.wait()
    bulk_wait(dv_rcv, nst - 1, rsem.at[DV])
    owner_sum(dv_rcv, run, pas_v)
    own_xv = send_x(pas_v, own_v, XV)

    tile = 256
    pv_t = pas_v[...].reshape(rows, heads * HD).T

    @pl.loop(0, width // tile)
    def _(j):
        at = pl.multiple_of(j * tile, tile)
        part = dot(pv_t, normed[:, pl.ds(at, tile)]).T
        gw_full[pl.ds(j * (tile // gw_full.shape[1]), tile // gw_full.shape[1])] = part.reshape(
            tile // gw_full.shape[1], gw_full.shape[1], heads * HD
        )

    other = lax.rem(c + 1, nc)
    gw_by = gw_full.reshape(nz * ny, nc, gw_full.shape[1], heads * HD)
    to_core = pltpu.make_async_remote_copy(
        src_ref=gw_by.at[:, other],
        dst_ref=gwc_rcv,
        send_sem=ssem.at[GC],
        recv_sem=rsem.at[GC],
        device_id=(z, y, other, x),
        device_id_type=MESH,
    )
    to_core.start()

    to_core.wait()

    @pl.loop(0, nz * ny)
    def _(i):
        zi, yi = i // ny, lax.rem(i, ny)
        gwy[yi, zi] = (gw_full[i * nc + c] + gwc_rcv[i]).astype(BF)

    @pl.loop(1, ny)
    def _(i):
        py = lax.rem(y + i, ny)
        pltpu.make_async_remote_copy(
            src_ref=gwy.at[py],
            dst_ref=gwy_rcv.at[i],
            send_sem=ssem.at[GY],
            recv_sem=rsem.at[GY],
            device_id=(z, py, c, x),
            device_id_type=MESH,
        ).start()

    send_piece(1)
    send_piece(2)

    bulk_wait(wk_all, nx - 1, rsem.at[WK])
    bulk_wait(wv_all, nx - 1, rsem.at[WV])
    own_xv.wait()
    bulk_wait(own_v, nx - 1, rsem.at[XV])

    @pl.loop(0, width // tile)
    def _(j):
        at = pl.ds(pl.multiple_of(j * tile, tile), tile)
        acc = dot(own_v[0].reshape(quarter, heads * HD), wv_all[0, at, :], NT)
        for s in range(1, nx):
            acc += dot(own_v[s].reshape(quarter, heads * HD), wv_all[s, at, :], NT)
        acc = acc.reshape(few, 2, half, tile)
        gn[0, :, at] = acc[:, 0].reshape(few * half, tile)
        gn[1, :, at] = acc[:, 1].reshape(few * half, tile)

    def keys_piece(k):
        part, cols = pieces[k]
        own = pltpu.make_async_copy(dk_snd[k].at[me], dk_rcv[k].at[me], self_sem.at[DK + k])
        own.wait()
        bulk_wait(dk_rcv[k], nst - 1, rsem.at[DK + k])
        bulk_wait(dk_snd[k], nst - 1, ssem.at[DK + k])
        owner_sum(dk_rcv[k], dk_snd[k], pas_k[k])
        own_x = send_x(pas_k[k], own_k[k], XK + k)
        own_x.wait()
        bulk_wait(own_k[k], nx - 1, rsem.at[XK + k])

        @pl.loop(0, width // tile)
        def _(j):
            at = pl.ds(pl.multiple_of(j * tile, tile), tile)
            acc = gn[part, :, at]
            for s in range(nx):
                mine = own_k[k][s].reshape(few * half, cols.stop - cols.start)
                acc += dot(mine, wk_all[s, at, cols], NT)
            gn[part, :, at] = acc

    def finish(part):
        @pl.loop(0, few)
        def _(j):
            at = pl.ds(pl.multiple_of(j * PLEN + part * half, half), half)
            first = x * quarter + j * PLEN + part * half
            s = store[pl.ds(pl.multiple_of(first, half), half), :].astype(F32)
            r = lax.rsqrt(jnp.mean(s * s, axis=-1, keepdims=True) + EPS)
            u = s * r
            g = gn[part, pl.ds(pl.multiple_of(j * half, half), half), :] * gain_ref[...]
            gs_ref[at, :] = (r * (g - u * jnp.mean(g * u, axis=-1, keepdims=True))).astype(BF)

    keys_piece(0)
    bulk_wait(gwy, ny - 1, ssem.at[GY])
    bulk_wait(gwy_rcv, ny - 1, rsem.at[GY])

    @pl.loop(0, nz)
    def _(i):
        acc = gwy[y, i].astype(F32)
        for j in range(1, ny):
            acc += gwy_rcv[j, i].astype(F32)
        gwz[i] = acc.astype(BF)

    @pl.loop(1, nz)
    def _(i):
        pz = lax.rem(z + i, nz)
        pltpu.make_async_remote_copy(
            src_ref=gwz.at[pz],
            dst_ref=gwz_rcv.at[i],
            send_sem=ssem.at[GZ],
            recv_sem=rsem.at[GZ],
            device_id=(pz, y, c, x),
            device_id_type=MESH,
        ).start()

    finish(0)
    keys_piece(1)
    keys_piece(2)
    finish(1)
    bulk_wait(gwz, nz - 1, ssem.at[GZ])
    bulk_wait(gwz_rcv, nz - 1, rsem.at[GZ])
    acc = gwz[z].astype(F32)
    for j in range(1, nz):
        acc += gwz_rcv[j].astype(F32)
    gw_ref[...] = acc

    bulk_wait(asked_v, nst - 1, ssem.at[REQ])
    bulk_wait(snd_b, nst - 1, ssem.at[V])
    bulk_wait(snd_a, nst - 1, ssem.at[DV])
    for k in range(3):
        bulk_wait(own_k[k], nx - 1, ssem.at[XK + k])
    bulk_wait(wk_all, nx - 1, ssem.at[WK])
    bulk_wait(wv_all, nx - 1, ssem.at[WV])
    bulk_wait(own_v, nx - 1, ssem.at[XV])


def widen_kernel(*refs):
    half = len(refs) // 2
    for src, dst in zip(refs[:half], refs[half:]):
        dst[...] = src[...].astype(F32)


def widened(arrays, steps):
    specs = [pl.BlockSpec((a.shape[0] // steps, a.shape[1]), lambda i: (i, 0)) for a in arrays]
    return pl.pallas_call(
        widen_kernel,
        grid=(steps,),
        out_shape=tuple(jax.ShapeDtypeStruct(a.shape, F32) for a in arrays),
        in_specs=specs,
        out_specs=tuple(specs),
    )(*arrays)


def local(dims, queries, gate_pre, cotangent, store, store_gain, w_key, w_value, owners, slots):
    nz, ny, nc, nx = dims
    nst = nz * ny * nc
    blocks, per = owners.shape
    rows, width = store.shape
    tokens, cols = queries.shape
    heads = cols // HD
    npass = rows // PLEN
    count = blocks * per
    quarter = rows // nx
    piece = width // nst
    anywhere = pl.BlockSpec(memory_space=pl.ANY)
    vmem = pl.BlockSpec(memory_space=pltpu.VMEM)
    per_peer = pltpu.VMEM((nst, PLEN, cols), BF)
    half = PLEN // 2
    few = npass // nx
    wide = pltpu.VMEM((nst, half, cols), BF)
    narrow = pltpu.VMEM((nst, half, HD), BF)
    dq, gs, gw = pl.pallas_call(
        functools.partial(kernel, (nz, ny, nc, nx, npass)),
        out_shape=(
            jax.ShapeDtypeStruct((tokens, cols), BF),
            jax.ShapeDtypeStruct((quarter, width), BF),
            jax.ShapeDtypeStruct((piece, cols), F32),
        ),
        in_specs=[anywhere] * 9,
        out_specs=(vmem, vmem, vmem),
        scratch_shapes=[
            pltpu.VMEM((rows, width), BF),
            pltpu.VMEM((rows, width), BF),
            pltpu.VMEM((nx, width, cols), BF),
            pltpu.VMEM((nx, width, cols), BF),
            pltpu.VMEM((tokens, cols), BF),
            pltpu.VMEM((tokens, cols), BF),
            pltpu.VMEM((tokens, cols), BF),
            pltpu.VMEM((npass, PLEN, cols), BF),
            per_peer,
            per_peer,
            per_peer,
            per_peer,
            per_peer,
            wide,
            narrow,
            narrow,
            wide,
            narrow,
            narrow,
            pltpu.VMEM((blocks * heads, per * PLEN, 128), F32),
            pltpu.VMEM((count, PLEN, cols), BF),
            per_peer,
            pltpu.VMEM((npass, PLEN, cols), BF),
            pltpu.VMEM((npass, half, cols), BF),
            pltpu.VMEM((npass, half, HD), BF),
            pltpu.VMEM((npass, half, HD), BF),
            pltpu.VMEM((nx, few, PLEN, cols), BF),
            pltpu.VMEM((nx, few, half, cols), BF),
            pltpu.VMEM((nx, few, half, HD), BF),
            pltpu.VMEM((nx, few, half, HD), BF),
            pltpu.VMEM((2, few * half, width), F32),
            pltpu.VMEM((nst, piece, cols), F32),
            pltpu.VMEM((nz * ny, piece, cols), F32),
            pltpu.VMEM((ny, nz, piece, cols), BF),
            pltpu.VMEM((ny, nz, piece, cols), BF),
            pltpu.VMEM((nz, piece, cols), BF),
            pltpu.VMEM((nz, piece, cols), BF),
            pltpu.VMEM((nst, 1, 128), jnp.int32),
            pltpu.VMEM((nst, 1, 128), jnp.int32),
            pltpu.VMEM((8, 128), jnp.int32),
            pltpu.SMEM((8, 128), jnp.int32),
            pltpu.VMEM((1, width), F32),
            pltpu.SMEM((per, blocks), jnp.int32),
            pltpu.SMEM((per, blocks), jnp.int32),
            pltpu.SemaphoreType.DMA((14,)),
            pltpu.SemaphoreType.DMA((16,)),
            pltpu.SemaphoreType.DMA((16,)),
            pltpu.SemaphoreType.DMA((16,)),
        ],
        compiler_params=pltpu.CompilerParams(
            collective_id=0, has_side_effects=True, vmem_limit_bytes=67_043_328
        ),
    )(
        store,
        w_key,
        w_value,
        queries,
        gate_pre,
        cotangent,
        store_gain.reshape(1, width),
        owners.T,
        slots.T,
    )
    return widened((dq, gs, gw), 4)


def solution(mesh):
    nx = mesh.shape["tp"]
    nst = mesh.shape["st"]
    nz, ny, nc = nst // 8, 4, 2
    torus = Mesh(mesh.devices.reshape(nz, ny, nc, nx), ST_TP)
    return jax.shard_map(
        functools.partial(local, (nz, ny, nc, nx)),
        mesh=torus,
        in_specs=(
            P(ST, "tp"),
            P(ST, "tp"),
            P(ST, "tp"),
            P(ST, None),
            P(),
            P(None, "tp"),
            P(None, "tp"),
            P(ST, None),
            P(ST, None),
        ),
        out_specs=(P(ST, "tp"), P(ST_TP, None), P(ST, "tp")),
        check_vma=False,
    )
```
